512 devices in a mesh: rep: 2 (over z_hi), fs: 32 (over z_lo, y), tp: 8 (over x, core).
Axes of the slice: x: 4, y: 4, z: 16 (z_hi: 2, z_lo: 8; z = z_hi * 8 + z_lo), core: 2. Of those that a mesh axis runs over, the one named last changes fastest.
Arguments:
- tokens: bfloat16 [32768, 2048], P(('rep', 'fs')), may hold values from -6 to 6
- mix_gain: float32 [2048], replicated, may hold values from 0.1 to 1.9
- gate_proj: bfloat16 [2048, 1024], P('fs', 'tp'), may hold values from -0.125 to 0.125
- value_proj: bfloat16 [2048, 1024], P('fs', 'tp'), may hold values from -0.125 to 0.125
- value_gain: float32 [1024], P('tp'), may hold values from 0.1 to 1.9
- value_shift: float32 [1024], P('tp'), may hold values from -3 to 3
- spatial_weight: bfloat16 [4, 128, 128], replicated, may hold values from -0.5 to 0.5
- spatial_shift: float32 [4, 128], replicated, may hold values from 0.1 to 1.9
- out_proj: bfloat16 [1024, 2048], P('tp', 'fs'), may hold values from -0.1875 to 0.1875
- ffn_gain: float32 [2048], replicated, may hold values from 0.1 to 1.9
- up_proj: bfloat16 [2048, 8192], P('fs', 'tp'), may hold values from -0.125 to 0.125
- down_proj: bfloat16 [8192, 2048], P('tp', 'fs'), may hold values from -0.0625 to 0.0625
Outputs:
- layer_out: bfloat16 [32768, 2048], P(('rep', 'fs'))
The draws below stay inside these ranges and needn't reach their ends.
All inputs are finite; a program needn't handle non-finite values.
Results may differ from the reference program's by a relative error of at most 0.018.
Values may be sent and summed in bfloat16 or wider, within the bound.
No kernel may reach another device: no remote copies, remote signals or barrier semaphores. Data moves between devices by JAX's collectives and lax.ppermute only.
A program may use at most 128 MiB of HBM per device.

```python
import jax
import jax.numpy as jnp
from jax import lax

D = 2048
GW = 1024
GROUPS = 4
BLOCK = 128
FF = 8192
TOKENS = 32768
N_TP = 8


def shard_levels(stream_key, extent, cuts, low, high):
    def one(axis_at, blocks):
        heights = jax.random.uniform(jax.random.fold_in(jax.random.fold_in(stream_key, 6), axis_at), (blocks,), jnp.float32, low / len(cuts), high / len(cuts))
        return jnp.repeat(jnp.exp(heights), extent[axis_at] // blocks).reshape((-1,) + (1,) * (len(extent) - axis_at - 1))

    gain = one(*cuts[0])
    for cut in cuts[1:]:
        gain = gain * one(*cut)
    return gain


def gaussian(key, dims, width, reach, split=(), kind=jnp.bfloat16):
    entries = jax.random.normal(key, dims, jnp.float32) * width
    if len(split) > 0:
        entries = shard_levels(key, dims, split, -0.22, 0.18) * entries
    return jnp.clip(entries, min=-reach, max=reach).astype(kind)


def setup_inputs(seed: int = 0) -> dict:
    streams_of = jax.random.split(jax.random.key(seed), 13)
    return {
        "tokens": gaussian(streams_of[0], (TOKENS, D), 1.0, 6.0, ((0, 64),)),
        "mix_gain": jnp.clip(1.0 + 0.18 * jax.random.normal(streams_of[1], (D,), jnp.float32), 0.1, 1.9),
        "gate_proj": gaussian(streams_of[2], (D, GW), D ** -0.5, 0.125, ((0, 32), (1, 8))),
        "value_proj": gaussian(streams_of[3], (D, GW), D ** -0.5, 0.125, ((0, 32), (1, 8))),
        "value_gain": jnp.clip(1.0 + 0.18 * jax.random.normal(streams_of[4], (GW,), jnp.float32), 0.1, 1.9),
        "value_shift": gaussian(streams_of[5], (GW,), 0.5, 3.0, ((0, 8),), jnp.float32),
        "spatial_weight": gaussian(streams_of[6], (GROUPS, BLOCK, BLOCK), BLOCK ** -0.5, 0.5),
        "spatial_shift": jnp.clip(1.0 + 0.18 * jax.random.normal(streams_of[7], (GROUPS, BLOCK), jnp.float32), 0.1, 1.9),
        "out_proj": gaussian(streams_of[8], (GW, D), GW ** -0.5, 0.1875, ((0, 8), (1, 32))),
        "ffn_gain": jnp.clip(1.0 + 0.18 * jax.random.normal(streams_of[9], (D,), jnp.float32), 0.1, 1.9),
        "up_proj": gaussian(streams_of[10], (D, FF), D ** -0.5, 0.125, ((0, 32), (1, 8))),
        "down_proj": gaussian(streams_of[11], (FF, D), FF ** -0.5, 0.0625, ((0, 8), (1, 32))),
    }


EPS = 1e-06

def rms_norm(values, scale):
    floats = values.astype(jnp.float32)
    return (floats * lax.rsqrt(lax.optimization_barrier(jnp.mean(floats * floats, axis=-1, keepdims=True)) + EPS) * scale).astype(jnp.bfloat16)

def blocked_sum(left, right):
    rows = left.shape[0]
    inner = left.shape[1] // N_TP
    left_blocks = left.reshape(rows, N_TP, inner).transpose(1, 0, 2)
    right_blocks = right.reshape(N_TP, inner, right.shape[1])

    def step(total, pair):
        term = jnp.dot(pair[0], pair[1], preferred_element_type=jnp.float32)
        term = lax.optimization_barrier(term.astype(jnp.bfloat16)).astype(jnp.float32)
        return (total + term, None)
    start = jnp.zeros((rows, right.shape[1]), jnp.float32)
    total, unused = lax.scan(step, start, (left_blocks, right_blocks))
    return total

def reference(tokens, mix_gain, gate_proj, value_proj, value_gain, value_shift, spatial_weight, spatial_shift, out_proj, ffn_gain, up_proj, down_proj):
    rows = tokens.shape[0]
    normed = rms_norm(tokens, mix_gain)
    gate = jax.nn.gelu(jnp.dot(normed, gate_proj, preferred_element_type=jnp.float32))
    value = jax.nn.gelu(jnp.dot(normed, value_proj, preferred_element_type=jnp.float32))
    centre = lax.optimization_barrier(jnp.mean(value, axis=-1, keepdims=True))
    spread = lax.optimization_barrier(jnp.mean(value * value, axis=-1, keepdims=True)) - centre * centre
    leveled = ((value - centre) * lax.rsqrt(spread + EPS) * value_gain + value_shift).astype(jnp.bfloat16)
    lower = jnp.tril(spatial_weight).astype(jnp.float32)
    pieces = leveled.reshape(rows // BLOCK, BLOCK, GROUPS, GW // GROUPS).astype(jnp.float32)
    mixed = jnp.einsum('gts,nsgw->ntgw', lower, pieces) + spatial_shift.T[None, :, :, None]
    gated = (gate * mixed.reshape(rows, GW)).astype(jnp.bfloat16)
    midway = (tokens.astype(jnp.float32) + blocked_sum(gated, out_proj)).astype(jnp.bfloat16)
    normed2 = rms_norm(midway, ffn_gain)
    hidden = jnp.square(jax.nn.relu(jnp.dot(normed2, up_proj, preferred_element_type=jnp.float32))).astype(jnp.bfloat16)
    return (midway.astype(jnp.float32) + blocked_sum(hidden, down_proj)).astype(jnp.bfloat16)
```

```python
import jax
import jax.numpy as jnp
from jax import lax
from jax.sharding import Mesh
from jax.sharding import PartitionSpec as P

GW = 1024
GROUPS = 4
BLOCK = 128
EPS = 1e-06
FS = ("zl", "y")
TP = ("x", "c")
REP_FS = ("zh", "zl", "y")
NZ, NY, NX = 8, 4, 4


def rms_norm(values, scale):
    floats = values.astype(jnp.float32)
    return (
        floats * lax.rsqrt(jnp.mean(floats * floats, axis=-1, keepdims=True) + EPS) * scale
    ).astype(jnp.bfloat16)


def everyone(part, axis, size):
    return lax.all_to_all(jnp.broadcast_to(part[None], (size, *part.shape)), axis, 0, 0, tiled=True)


def gather_y(part):
    return everyone(part, "y", NY).reshape(NY * part.shape[0], part.shape[1])


def shift_z(part, by):
    around = 2 * NZ
    return lax.ppermute(part, ("zh", "zl"), [(i, (i + by) % around) for i in range(around)])


def ring_z(part):
    held = [None] * NZ
    held[0] = part
    up = down = part
    for k in range(1, 5):
        up = shift_z(up, 1)
        held[NZ - k] = up
        if k < 4:
            down = shift_z(down, -1)
            held[k] = down
    return held


def swap(part):
    return lax.ppermute(part, "c", [(0, 1), (1, 0)])


def turned(array, by):
    width = array.shape[-1]
    twice = jnp.concatenate([array, array], axis=-1)
    return lax.dynamic_slice_in_dim(twice, by, width, array.ndim - 1)


def body(
    tokens,
    mix_gain,
    gate_proj,
    value_proj,
    value_gain,
    value_shift,
    spatial_weight,
    spatial_shift,
    out_proj,
    ffn_gain,
    up_proj,
    down_proj,
):
    x, c, z = lax.axis_index("x"), lax.axis_index("c"), lax.axis_index("zl")
    rows = tokens.shape[0] // 2
    width = tokens.shape[1]
    chunk = rows // NX
    block = width // NZ

    small = gather_y(jnp.concatenate([gate_proj, value_proj, out_proj.T], axis=1))
    small_rel = jnp.concatenate(ring_z(small), axis=0)
    small_pair = swap(small_rel)
    large = gather_y(jnp.concatenate([up_proj, down_proj.T], axis=1))
    large_rel = jnp.concatenate(ring_z(large), axis=0)
    large_pair = swap(large_rel)

    mine = lax.dynamic_slice_in_dim(tokens, c * rows, rows, 0)
    mine = turned(mine, z * block)
    mix_rel = turned(mix_gain, z * block)
    ffn_rel = turned(ffn_gain, z * block)
    affine = jnp.stack([value_gain, value_shift])
    affine = jnp.concatenate([affine, swap(affine)], axis=1)

    normed = rms_norm(mine, mix_rel)
    n = gate_proj.shape[1]
    gate_w = jnp.concatenate([small_rel[:, :n], small_pair[:, :n]], axis=1)
    value_w = jnp.concatenate([small_rel[:, n : 2 * n], small_pair[:, n : 2 * n]], axis=1)
    gate = jax.nn.gelu(jnp.dot(normed, gate_w, preferred_element_type=jnp.float32))
    value = jax.nn.gelu(jnp.dot(normed, value_w, preferred_element_type=jnp.float32))
    stats = jnp.stack([jnp.sum(value, axis=-1), jnp.sum(value * value, axis=-1)])
    stats = jnp.sum(everyone(stats, "x", NX), axis=0)
    centre = (stats[0] / GW)[:, None]
    spread = (stats[1] / GW)[:, None] - centre * centre
    leveled = ((value - centre) * lax.rsqrt(spread + EPS) * affine[0] + affine[1]).astype(jnp.bfloat16)
    lower = jnp.tril(lax.dynamic_index_in_dim(spatial_weight, x, 0, keepdims=False))
    offset = lax.dynamic_index_in_dim(spatial_shift, x, 0, keepdims=False)
    pieces = leveled.reshape(rows // BLOCK, BLOCK, 2 * n)
    mixed = (
        jnp.einsum("ts,nsw->ntw", lower, pieces, preferred_element_type=jnp.float32)
        + offset[None, :, None]
    )
    gated = (gate * mixed.reshape(rows, 2 * n)).astype(jnp.bfloat16)
    out_w = jnp.concatenate([small_rel[:, 2 * n :], small_pair[:, 2 * n :]], axis=1)
    mixer = lax.dot_general(gated, out_w, (((1,), (1,)), ((), ())), preferred_element_type=jnp.float32)
    mixer = mixer.astype(jnp.bfloat16).reshape(NX, chunk, width)
    mixer = jnp.sum(lax.all_to_all(mixer, "x", 0, 0, tiled=True).astype(jnp.float32), axis=0)
    base = lax.dynamic_slice_in_dim(mine, x * chunk, chunk, 0)
    midway = (base.astype(jnp.float32) + mixer).astype(jnp.bfloat16)
    normed2 = everyone(rms_norm(midway, ffn_rel), "x", NX).reshape(rows, width)

    f = up_proj.shape[1]
    hidden = []
    for w in (large_rel, large_pair):
        acc = jnp.dot(normed2, w[:, :f], preferred_element_type=jnp.float32)
        hidden.append(jnp.square(jax.nn.relu(acc)).astype(jnp.bfloat16))
    terms = sum(
        lax.dot_general(h, w[:, f:], (((1,), (1,)), ((), ())), preferred_element_type=jnp.float32)
        for h, w in zip(hidden, (large_rel, large_pair))
    )
    terms = terms.astype(jnp.bfloat16).reshape(NX, chunk, width)
    ffn = jnp.sum(lax.all_to_all(terms, "x", 0, 0, tiled=True).astype(jnp.float32), axis=0)
    done = (midway.astype(jnp.float32) + ffn).astype(jnp.bfloat16)
    done = turned(done, (NZ - z) * block)
    done = everyone(done, "x", NX).reshape(rows, width)
    return everyone(done, "c", 2).reshape(2 * rows, width)


def solution(mesh):
    finer = Mesh(
        mesh.devices.reshape(mesh.shape["rep"], NZ, NY, NX, 2), ("zh", "zl", "y", "x", "c")
    )
    placed = (
        P(REP_FS, None),
        P(),
        P(FS, TP),
        P(FS, TP),
        P(TP),
        P(TP),
        P(),
        P(),
        P(TP, FS),
        P(),
        P(FS, TP),
        P(TP, FS),
    )
    return jax.shard_map(
        body, mesh=finer, in_specs=placed, out_specs=P(REP_FS, None), check_vma=False
    )
```

```python
import jax
import jax.numpy as jnp
from jax import lax
from jax.sharding import Mesh
from jax.sharding import PartitionSpec as P

GW = 1024
BLOCK = 128
EPS = 1e-06
FS = ("zl", "y")
TP = ("x", "c")
REP_FS = ("zh", "zl", "y")
NZ, NY, NX = 8, 4, 4


def rms_norm(values, scale):
    floats = values.astype(jnp.float32)
    return (
        floats * lax.rsqrt(jnp.mean(floats * floats, axis=-1, keepdims=True) + EPS) * scale
    ).astype(jnp.bfloat16)


def everyone(part, axis, size):
    return lax.all_to_all(jnp.broadcast_to(part[None], (size, *part.shape)), axis, 0, 0, tiled=True)


def shift_z(part, by):
    around = 2 * NZ
    return lax.ppermute(part, ("zh", "zl"), [(i, (i + by) % around) for i in range(around)])


def swap(part):
    return lax.ppermute(part, "c", [(0, 1), (1, 0)])


def y_major(array):
    k = array.shape[-1] // (NZ * NY)
    starts = [(z * NY + y) * k for y in range(NY) for z in range(NZ)]
    return jnp.concatenate([array[..., s : s + k] for s in starts], axis=-1)


def z_major(array):
    k = array.shape[-1] // (NZ * NY)
    starts = [(y * NZ + z) * k for z in range(NZ) for y in range(NY)]
    return jnp.concatenate([array[..., s : s + k] for s in starts], axis=-1)


def placed_z(pieces, z, dim, shape):
    whole = jnp.zeros(shape, jnp.bfloat16)
    for offset, piece in pieces:
        at = [0] * len(shape)
        at[dim] = lax.rem(z + offset, NZ)
        whole = lax.dynamic_update_slice(whole, jnp.expand_dims(piece, dim), at)
    return whole


def around_z(pair, dim):
    near = lambda a: lax.index_in_dim(a, 0, dim, keepdims=False)
    far = lambda a: lax.index_in_dim(a, 1, dim, keepdims=False)
    low, high = shift_z(pair, 1), shift_z(pair, -1)
    low2, high2 = shift_z(near(low), 1), shift_z(near(high), -1)
    return [
        (0, near(pair)), (4, far(pair)), (7, near(low)), (3, far(low)),
        (1, near(high)), (5, far(high)), (6, low2), (2, high2),
    ]


def body(
    tokens,
    mix_gain,
    gate_proj,
    value_proj,
    value_gain,
    value_shift,
    spatial_weight,
    spatial_shift,
    out_proj,
    ffn_gain,
    up_proj,
    down_proj,
):
    x, c, z = lax.axis_index("x"), lax.axis_index("c"), lax.axis_index("zl")
    rows = tokens.shape[0] // 2
    width = tokens.shape[1]
    chunk = rows // NX
    k, n = gate_proj.shape
    f = up_proj.shape[1]

    def small(part):
        whole = everyone(everyone(part, "zl", NZ), "y", NY).reshape(width, n)
        return whole, swap(whole)

    value_w = small(value_proj)
    gate_w = small(gate_proj)
    out_w = small(out_proj.T)

    near = jnp.stack([up_proj, down_proj.T])
    far = shift_z(near, 4)
    down = around_z(jnp.stack([near[1], far[1]]), 0)
    down = everyone(placed_z(down, z, 0, (NZ, k, f)), "y", NY).reshape(width, f)
    down_w = (down, swap(down))
    up = around_z(everyone(jnp.stack([near[0], far[0]]), "y", NY), 1)
    up = placed_z(up, z, 1, (NY, NZ, k, f)).reshape(width, f)
    up_w = (up, swap(up))

    mine = y_major(lax.dynamic_slice_in_dim(tokens, c * rows, rows, 0))
    affine = jnp.stack([value_gain, value_shift])
    affine = jnp.concatenate([affine, swap(affine)], axis=1)

    normed = rms_norm(mine, y_major(mix_gain))
    value = jnp.concatenate(
        [jax.nn.gelu(jnp.dot(normed, w, preferred_element_type=jnp.float32)) for w in value_w], axis=1
    )
    gate = jnp.concatenate(
        [jax.nn.gelu(jnp.dot(normed, w, preferred_element_type=jnp.float32)) for w in gate_w], axis=1
    )
    stats = jnp.stack([jnp.sum(value, axis=-1), jnp.sum(value * value, axis=-1)])
    stats = jnp.sum(everyone(stats, "x", NX), axis=0)
    centre = (stats[0] / GW)[:, None]
    spread = (stats[1] / GW)[:, None] - centre * centre
    leveled = ((value - centre) * lax.rsqrt(spread + EPS) * affine[0] + affine[1]).astype(jnp.bfloat16)
    lower = jnp.tril(lax.dynamic_index_in_dim(spatial_weight, x, 0, keepdims=False))
    offset = lax.dynamic_index_in_dim(spatial_shift, x, 0, keepdims=False)
    pieces = leveled.reshape(rows // BLOCK, BLOCK, 2 * n)
    mixed = (
        jnp.einsum("ts,nsw->ntw", lower, pieces, preferred_element_type=jnp.float32)
        + offset[None, :, None]
    )
    gated = (gate * mixed.reshape(rows, 2 * n)).astype(jnp.bfloat16)
    mixer = lax.dot_general(
        gated, jnp.concatenate(out_w, axis=1), (((1,), (1,)), ((), ())), preferred_element_type=jnp.float32
    )
    mixer = mixer.astype(jnp.bfloat16).reshape(NX, chunk, width)
    mixer = jnp.sum(lax.all_to_all(mixer, "x", 0, 0, tiled=True).astype(jnp.float32), axis=0)
    base = lax.dynamic_slice_in_dim(mine, x * chunk, chunk, 0)
    midway = (base.astype(jnp.float32) + mixer).astype(jnp.bfloat16)
    normed2 = everyone(rms_norm(midway, y_major(ffn_gain)), "x", NX).reshape(rows, width)

    terms = 0
    for up, down in zip(up_w, down_w):
        acc = jnp.dot(normed2, up, preferred_element_type=jnp.float32)
        hidden = jnp.square(jax.nn.relu(acc)).astype(jnp.bfloat16)
        terms += lax.dot_general(hidden, down, (((1,), (1,)), ((), ())), preferred_element_type=jnp.float32)
    terms = terms.astype(jnp.bfloat16).reshape(NX, chunk, width)
    ffn = jnp.sum(lax.all_to_all(terms, "x", 0, 0, tiled=True).astype(jnp.float32), axis=0)
    done = z_major((midway.astype(jnp.float32) + ffn).astype(jnp.bfloat16))
    done = everyone(done, "x", NX).reshape(rows, width)
    return everyone(done, "c", 2).reshape(2 * rows, width)


def solution(mesh):
    finer = Mesh(
        mesh.devices.reshape(mesh.shape["rep"], NZ, NY, NX, 2), ("zh", "zl", "y", "x", "c")
    )
    placed = (
        P(REP_FS, None),
        P(),
        P(FS, TP),
        P(FS, TP),
        P(TP),
        P(TP),
        P(),
        P(),
        P(TP, FS),
        P(),
        P(FS, TP),
        P(TP, FS),
    )
    return jax.shard_map(
        body, mesh=finer, in_specs=placed, out_specs=P(REP_FS, None), check_vma=False
    )
```

```python
import jax
import jax.numpy as jnp
from jax import lax
from jax.experimental import pallas as pl
from jax.experimental.pallas import tpu as pltpu
from jax.sharding import Mesh
from jax.sharding import PartitionSpec as P

GW = 1024
BLOCK = 128
EPS = 1e-06
FS = ("zl", "y")
TP = ("x", "c")
REP_FS = ("zh", "zl", "y")
NZ, NY, NX = 8, 4, 4
NT = (((1,), (1,)), ((), ()))


def rms_norm(values, scale):
    floats = values.astype(jnp.float32)
    return (
        floats * lax.rsqrt(jnp.mean(floats * floats, axis=-1, keepdims=True) + EPS) * scale
    ).astype(jnp.bfloat16)


def exchange(parts, axis):
    return lax.all_to_all(parts, axis, 0, 0, tiled=True)


def everyone(part, axis, size):
    return exchange(jnp.broadcast_to(part[None], (size, *part.shape)), axis)


def swap(part):
    return lax.ppermute(part, "c", [(0, 1), (1, 0)])


def shift_x(part, by):
    return lax.ppermute(part, "x", [(i, (i + by) % NX) for i in range(NX)])


FIRST = 2, 1, 3


def gather_x(part):
    found = {0: part}
    for d in FIRST:
        found[d] = shift_x(part, d)
    return [found[d] for d in range(NX)]


def reduce_x(parts, toward):
    found = {0: parts[0]}
    for d in FIRST:
        found[d] = shift_x(parts[d], toward * d)
    return sum(found[d].astype(jnp.float32) for d in range(NX))


def y_major(array):
    k = array.shape[-1] // (NZ * NY)
    starts = [(z * NY + y) * k for y in range(NY) for z in range(NZ)]
    return jnp.concatenate([array[..., s : s + k] for s in starts], axis=-1)


AROUND_Y = 0, 2, 3, 1


def around_y(part):
    moved = [part]
    for by in (2, 1, -1):
        moved.append(lax.ppermute(part, "y", [(i, (i + by) % NY) for i in range(NY)]))
    return moved


def pack_kernel(at_ref, *refs, slots):
    pieces, out, sem = refs[:-2], refs[-2], refs[-1]
    copies = []
    for i, piece in enumerate(pieces):
        target = out.at[slots(i, at_ref)]
        copies.append(pltpu.make_async_copy(piece, target, sem.at[i]))
        copies[-1].start()
    for copy in copies:
        copy.wait()


def pack(at, pieces, slots):
    count = len(pieces)
    shape = (count, *pieces[0].shape)
    return pl.pallas_call(
        lambda *refs: pack_kernel(*refs, slots=slots),
        out_shape=jax.ShapeDtypeStruct(shape, jnp.bfloat16),
        in_specs=[pl.BlockSpec(memory_space=pltpu.SMEM)]
        + [pl.BlockSpec(memory_space=pltpu.VMEM)] * count,
        out_specs=pl.BlockSpec(memory_space=pl.ANY),
        scratch_shapes=[pltpu.SemaphoreType.DMA((count,))],
        cost_estimate=pl.CostEstimate(
            flops=1_000_000_000, bytes_accessed=4 * count * pieces[0].size, transcendentals=0
        ),
    )(at, *pieces)


def y_slot(i, at_ref):
    return lax.rem(at_ref[0] + AROUND_Y[i], NY)


def row_slot(i, at_ref):
    core = at_ref[1] if i < NX else 1 - at_ref[1]
    return core * NX + lax.rem(at_ref[0] + NX - i % NX, NX)


def mixer_kernel(x_ref, w_ref, out, held, hidden, sem):
    f = w_ref.shape[2] // 2
    copies = []
    for side in range(2):
        for h in range(2):
            at = pl.ds(side * f, f)
            copy = pltpu.make_async_copy(w_ref.at[h, :, at], held.at[h, :, at], sem.at[side, h])
            copy.start()
            copies.append(copy)
    for h in range(2):
        copies[h].wait()
        acc = jnp.dot(x_ref[...], held[h, :, :f], preferred_element_type=jnp.float32)
        acc = jnp.maximum(acc, 0.0)
        hidden[h] = (acc * acc).astype(jnp.bfloat16)
    for copy in copies[2:]:
        copy.wait()
    width = out.shape[1]
    for at in range(0, width, 512):
        acc = None
        for h in range(2):
            term = lax.dot_general(
                hidden[h], held[h, at : at + 512, f:], NT, preferred_element_type=jnp.float32
            )
            acc = term if acc is None else acc + term
        out[:, at : at + 512] = acc.astype(jnp.bfloat16)


def channel_mixer(x, w):
    rows, width = x.shape
    f = w.shape[2] // 2
    return pl.pallas_call(
        mixer_kernel,
        out_shape=jax.ShapeDtypeStruct((rows, width), jnp.bfloat16),
        in_specs=[pl.BlockSpec(memory_space=pltpu.VMEM), pl.BlockSpec(memory_space=pltpu.HBM)],
        out_specs=pl.BlockSpec(memory_space=pltpu.VMEM),
        scratch_shapes=[
            pltpu.VMEM(w.shape, jnp.bfloat16),
            pltpu.VMEM((2, rows, f), jnp.bfloat16),
            pltpu.SemaphoreType.DMA((2, 2)),
        ],
        compiler_params=pltpu.CompilerParams(vmem_limit_bytes=30 * 1024 * 1024),
        cost_estimate=pl.CostEstimate(
            flops=8 * rows * width * f, bytes_accessed=2 * w.size, transcendentals=0
        ),
    )(x, w)


def body(
    tokens,
    mix_gain,
    gate_proj,
    value_proj,
    value_gain,
    value_shift,
    spatial_weight,
    spatial_shift,
    out_proj,
    ffn_gain,
    up_proj,
    down_proj,
):
    x, c = lax.axis_index("x"), lax.axis_index("c")
    at_y = jnp.reshape(lax.axis_index("y"), (1,)).astype(jnp.int32)
    rows = tokens.shape[0] // 2
    width = tokens.shape[1]
    chunk = rows // NX
    k, n = gate_proj.shape
    f = up_proj.shape[1]

    def small(part):
        whole = everyone(everyone(part, "zl", NZ), "y", NY)
        whole = whole.reshape(width, part.shape[1])
        return whole, swap(whole)

    small_w = small(jnp.concatenate([value_proj, gate_proj, out_proj.T], axis=1))

    half = f // 2
    at_half = lax.axis_index("zh") * half
    part = jnp.concatenate(
        [
            lax.dynamic_slice_in_dim(up_proj, at_half, half, 1),
            lax.dynamic_slice_in_dim(down_proj, at_half, half, 0).T,
        ],
        axis=1,
    )
    block = pack(at_y, around_y(part), y_slot).reshape(NY * k, f)
    large = lax.all_gather(block, ("zh", "zl"), axis=0, tiled=True).reshape(2, width, f)

    mine = lax.dynamic_slice_in_dim(tokens, c * rows, rows, 0)
    affine = jnp.stack([value_gain, value_shift])
    affine = jnp.concatenate([affine, swap(affine)], axis=1)

    normed = rms_norm(y_major(mine), y_major(mix_gain))
    value = jnp.concatenate(
        [jax.nn.gelu(jnp.dot(normed, w[:, :n], preferred_element_type=jnp.float32)) for w in small_w], axis=1
    )
    stats = jnp.stack([jnp.sum(value, axis=-1), jnp.sum(value * value, axis=-1)])
    stats = jnp.sum(everyone(stats, "x", NX), axis=0)
    gate = jnp.concatenate(
        [jax.nn.gelu(jnp.dot(normed, w[:, n : 2 * n], preferred_element_type=jnp.float32)) for w in small_w],
        axis=1,
    )
    centre = (stats[0] / GW)[:, None]
    spread = (stats[1] / GW)[:, None] - centre * centre
    leveled = ((value - centre) * lax.rsqrt(spread + EPS) * affine[0] + affine[1]).astype(jnp.bfloat16)
    lower = jnp.tril(lax.dynamic_index_in_dim(spatial_weight, x, 0, keepdims=False))
    offset = lax.dynamic_index_in_dim(spatial_shift, x, 0, keepdims=False)
    pieces = leveled.reshape(rows // BLOCK, BLOCK, 2 * n)
    mixed = (
        jnp.einsum("ts,nsw->ntw", lower, pieces, preferred_element_type=jnp.float32)
        + offset[None, :, None]
    )
    gated = (gate * mixed.reshape(rows, 2 * n)).astype(jnp.bfloat16)
    gated = lax.dynamic_slice_in_dim(jnp.concatenate([gated, gated[:-chunk]]), x * chunk, rows, 0)
    out_w = jnp.concatenate([w[:, 2 * n :] for w in small_w], axis=1)
    out_w = out_w.reshape(NY, NZ, k, 2 * n).transpose(1, 0, 2, 3).reshape(width, 2 * n)
    mixer = lax.dot_general(gated, out_w, NT, preferred_element_type=jnp.float32)
    mixer = mixer.astype(jnp.bfloat16).reshape(NX, chunk, width)
    base = lax.dynamic_slice_in_dim(mine, x * chunk, chunk, 0)
    midway = (base.astype(jnp.float32) + reduce_x(mixer, 1)).astype(jnp.bfloat16)
    normed2 = jnp.concatenate(gather_x(rms_norm(midway, ffn_gain)), axis=0)

    theirs = channel_mixer(swap(normed2), large)
    theirs = swap(theirs)
    terms = channel_mixer(normed2, large)
    terms = (terms.astype(jnp.float32) + theirs.astype(jnp.float32)).astype(jnp.bfloat16)
    ffn = reduce_x(terms.reshape(NX, chunk, width), -1)
    done = (midway.astype(jnp.float32) + ffn).astype(jnp.bfloat16)
    done = gather_x(done)
    done += [swap(part) for part in done]
    at_x = jnp.stack([x, c]).astype(jnp.int32)
    return pack(at_x, done, row_slot).reshape(2 * rows, width)


def solution(mesh):
    finer = Mesh(
        mesh.devices.reshape(mesh.shape["rep"], NZ, NY, NX, 2), ("zh", "zl", "y", "x", "c")
    )
    placed = (
        P(REP_FS, None),
        P(),
        P(FS, TP),
        P(FS, TP),
        P(TP),
        P(TP),
        P(),
        P(),
        P(TP, FS),
        P(),
        P(FS, TP),
        P(TP, FS),
    )

    return jax.shard_map(body, mesh=finer, in_specs=placed, out_specs=P(REP_FS, None), check_vma=False)
```

```python
import jax
import jax.numpy as jnp
from jax import lax
from jax.experimental import pallas as pl
from jax.experimental.pallas import tpu as pltpu
from jax.sharding import Mesh
from jax.sharding import PartitionSpec as P

GW = 1024
BLOCK = 128
EPS = 1e-06
FS = ("zl", "y")
TP = ("x", "c")
REP_FS = ("zh", "zl", "y")
NZ, NY, NX = 8, 4, 4
NT = (((1,), (1,)), ((), ()))


def rms_norm(values, scale):
    floats = values.astype(jnp.float32)
    return (
        floats * lax.rsqrt(jnp.mean(floats * floats, axis=-1, keepdims=True) + EPS) * scale
    ).astype(jnp.bfloat16)


def exchange(parts, axis):
    return lax.all_to_all(parts, axis, 0, 0, tiled=True)


def everyone(part, axis, size):
    return exchange(jnp.broadcast_to(part[None], (size, *part.shape)), axis)


def swap(part):
    return lax.ppermute(part, "c", [(0, 1), (1, 0)])


def y_major(array):
    k = array.shape[-1] // (NZ * NY)
    starts = [(z * NY + y) * k for y in range(NY) for z in range(NZ)]
    return jnp.concatenate([array[..., s : s + k] for s in starts], axis=-1)


def around_y(part):
    moved = [part]
    for by in (2, 1, -1):
        moved.append(lax.ppermute(part, "y", [(i, (i + by) % NY) for i in range(NY)]))
    return moved


def pack_kernel(at_ref, *refs, plan, size, times):
    pieces, out, sem = refs[:-2], refs[-2], refs[-1]
    copies = []
    for piece, source, offset in plan:
        ref = pieces[piece] if source is None else pieces[piece].at[source]
        slot = lax.rem(at_ref[0] + offset, size)
        for t in range(times):
            target = out.at[slot] if times == 1 else out.at[t, slot]
            copies.append(pltpu.make_async_copy(ref, target, sem.at[len(copies)]))
            copies[-1].start()
    for copy in copies:
        copy.wait()


def pack(at, pieces, plan, times):
    size = len(plan)
    shape = (size, *pieces[-1].shape) if times == 1 else (times, size, *pieces[-1].shape)
    moved = 2 * times * size * pieces[-1].size
    return pl.pallas_call(
        lambda *refs: pack_kernel(*refs, plan=plan, size=size, times=times),
        out_shape=jax.ShapeDtypeStruct(shape, jnp.bfloat16),
        in_specs=[pl.BlockSpec(memory_space=pltpu.SMEM)]
        + [pl.BlockSpec(memory_space=pltpu.VMEM)] * len(pieces),
        out_specs=pl.BlockSpec(memory_space=pl.ANY),
        scratch_shapes=[pltpu.SemaphoreType.DMA((size * times,))],
        cost_estimate=pl.CostEstimate(
            flops=1_000_000_000, bytes_accessed=2 * moved, transcendentals=0
        ),
    )(at, *pieces)


Y_PLAN = [(0, None, 0), (1, None, 2), (2, None, 3), (3, None, 1)]
Z_PLAN = [(0, 0, 0), (0, 1, 4), (1, 0, 7), (1, 1, 3), (2, 0, 1), (2, 1, 5), (3, None, 6), (4, None, 2)]


def shift_z(part, by):
    around = 2 * NZ
    return lax.ppermute(part, ("zh", "zl"), [(i, (i + by) % around) for i in range(around)])


def around_z(part):
    pair = jnp.stack([part, shift_z(part, 4)])
    low, high = shift_z(pair, 1), shift_z(pair, -1)
    return pair, low, high, shift_z(low[0], 1), shift_z(high[0], -1)


def mixer_kernel(x_ref, w_ref, out, hidden):
    f = w_ref.shape[2] // 2
    for h in range(2):
        acc = jnp.dot(x_ref[...], w_ref[h, :, :f], preferred_element_type=jnp.float32)
        acc = jnp.maximum(acc, 0.0)
        hidden[h] = (acc * acc).astype(jnp.bfloat16)
    width = out.shape[1]
    for at in range(0, width, 512):
        acc = None
        for h in range(2):
            term = lax.dot_general(
                hidden[h], w_ref[h, at : at + 512, f:], NT, preferred_element_type=jnp.float32
            )
            acc = term if acc is None else acc + term
        out[:, at : at + 512] = acc.astype(jnp.bfloat16)


def channel_mixer(x, w):
    rows, width = x.shape
    f = w.shape[2] // 2
    return pl.pallas_call(
        mixer_kernel,
        out_shape=jax.ShapeDtypeStruct((rows, width), jnp.bfloat16),
        in_specs=[pl.BlockSpec(memory_space=pltpu.VMEM)] * 2,
        out_specs=pl.BlockSpec(memory_space=pltpu.VMEM),
        scratch_shapes=[pltpu.VMEM((2, rows, f), jnp.bfloat16)],
        compiler_params=pltpu.CompilerParams(vmem_limit_bytes=30 * 1024 * 1024),
        cost_estimate=pl.CostEstimate(
            flops=8 * rows * width * f, bytes_accessed=2 * w.size, transcendentals=0
        ),
    )(x, w)


def body(
    tokens,
    mix_gain,
    gate_proj,
    value_proj,
    value_gain,
    value_shift,
    spatial_weight,
    spatial_shift,
    out_proj,
    ffn_gain,
    up_proj,
    down_proj,
):
    x, c = lax.axis_index("x"), lax.axis_index("c")
    at_z = jnp.reshape(lax.axis_index("zl"), (1,)).astype(jnp.int32)
    at_y = jnp.reshape(lax.axis_index("y"), (1,)).astype(jnp.int32)
    rows = tokens.shape[0] // 2
    width = tokens.shape[1]
    chunk = rows // NX
    k, n = gate_proj.shape
    f = up_proj.shape[1]

    part = jnp.concatenate([value_proj, gate_proj, out_proj.T], axis=1)
    small = exchange(pack(at_z, around_z(part), Z_PLAN, NY), "y")
    small = small.reshape(width, part.shape[1])
    small_w = (small, swap(small))

    half = f // 2
    at_half = lax.axis_index("zh") * half
    part = jnp.concatenate(
        [
            lax.dynamic_slice_in_dim(up_proj, at_half, half, 1),
            lax.dynamic_slice_in_dim(down_proj, at_half, half, 0).T,
        ],
        axis=1,
    )
    block = pack(at_y, around_y(part), Y_PLAN, 1).reshape(NY * k, f)
    large = lax.all_gather(block, ("zh", "zl"), axis=0, tiled=True).reshape(2, width, f)

    mine = lax.dynamic_slice_in_dim(tokens, c * rows, rows, 0)
    affine = jnp.stack([value_gain, value_shift])
    affine = jnp.concatenate([affine, swap(affine)], axis=1)

    normed = rms_norm(y_major(mine), y_major(mix_gain))
    value = jnp.concatenate(
        [jax.nn.gelu(jnp.dot(normed, w[:, :n], preferred_element_type=jnp.float32)) for w in small_w], axis=1
    )
    stats = jnp.stack([jnp.sum(value, axis=-1), jnp.sum(value * value, axis=-1)])
    stats = jnp.sum(everyone(stats, "x", NX), axis=0)
    gate = jnp.concatenate(
        [jax.nn.gelu(jnp.dot(normed, w[:, n : 2 * n], preferred_element_type=jnp.float32)) for w in small_w],
        axis=1,
    )
    centre = (stats[0] / GW)[:, None]
    spread = (stats[1] / GW)[:, None] - centre * centre
    leveled = ((value - centre) * lax.rsqrt(spread + EPS) * affine[0] + affine[1]).astype(jnp.bfloat16)
    lower = jnp.tril(lax.dynamic_index_in_dim(spatial_weight, x, 0, keepdims=False))
    offset = lax.dynamic_index_in_dim(spatial_shift, x, 0, keepdims=False)
    pieces = leveled.reshape(rows // BLOCK, BLOCK, 2 * n)
    mixed = (
        jnp.einsum("ts,nsw->ntw", lower, pieces, preferred_element_type=jnp.float32)
        + offset[None, :, None]
    )
    gated = (gate * mixed.reshape(rows, 2 * n)).astype(jnp.bfloat16)
    out_w = jnp.concatenate([w[:, 2 * n :] for w in small_w], axis=1)
    out_w = out_w.reshape(NY, NZ, k, 2 * n).transpose(1, 0, 2, 3).reshape(width, 2 * n)
    mixer = lax.dot_general(gated, out_w, NT, preferred_element_type=jnp.float32)
    mixer = mixer.astype(jnp.bfloat16).reshape(NX, chunk, width)
    mixer = jnp.sum(exchange(mixer, "x").astype(jnp.float32), axis=0)
    base = lax.dynamic_slice_in_dim(mine, x * chunk, chunk, 0)
    midway = (base.astype(jnp.float32) + mixer).astype(jnp.bfloat16)
    normed2 = everyone(rms_norm(midway, ffn_gain), "x", NX).reshape(rows, width)

    theirs = channel_mixer(swap(normed2), large)
    theirs = swap(theirs)
    terms = channel_mixer(normed2, large)
    terms = (terms.astype(jnp.float32) + theirs.astype(jnp.float32)).astype(jnp.bfloat16)
    ffn = jnp.sum(exchange(terms.reshape(NX, chunk, width), "x").astype(jnp.float32), axis=0)
    done = (midway.astype(jnp.float32) + ffn).astype(jnp.bfloat16)
    done = everyone(done, "x", NX).reshape(rows, width)
    return everyone(done, "c", 2).reshape(2 * rows, width)


def solution(mesh):
    finer = Mesh(
        mesh.devices.reshape(mesh.shape["rep"], NZ, NY, NX, 2), ("zh", "zl", "y", "x", "c")
    )
    placed = (
        P(REP_FS, None),
        P(),
        P(FS, TP),
        P(FS, TP),
        P(TP),
        P(TP),
        P(),
        P(),
        P(TP, FS),
        P(),
        P(FS, TP),
        P(TP, FS),
    )

    return jax.shard_map(body, mesh=finer, in_specs=placed, out_specs=P(REP_FS, None), check_vma=False)
```

```python
import jax
import jax.numpy as jnp
from jax import lax
from jax.experimental import pallas as pl
from jax.experimental.pallas import tpu as pltpu
from jax.sharding import Mesh
from jax.sharding import PartitionSpec as P

GW = 1024
BLOCK = 128
EPS = 1e-06
FS = ("zl", "y")
TP = ("x", "c")
REP_FS = ("zh", "zl", "y")
NZ, NY, NX = 8, 4, 4
NT = (((1,), (1,)), ((), ()))


def rms_norm(values, scale):
    floats = values.astype(jnp.float32)
    return (
        floats * lax.rsqrt(jnp.mean(floats * floats, axis=-1, keepdims=True) + EPS) * scale
    ).astype(jnp.bfloat16)


def exchange(parts, axis):
    return lax.all_to_all(parts, axis, 0, 0, tiled=True)


def everyone(part, axis, size):
    return exchange(jnp.broadcast_to(part[None], (size, *part.shape)), axis)


def swap(part):
    return lax.ppermute(part, "c", [(0, 1), (1, 0)])


def y_major(array):
    k = array.shape[-1] // (NZ * NY)
    starts = [(z * NY + y) * k for y in range(NY) for z in range(NZ)]
    return jnp.concatenate([array[..., s : s + k] for s in starts], axis=-1)


def pack_kernel(at_ref, *refs, plan, size, times):
    pieces, out, sem = refs[:-2], refs[-2], refs[-1]
    copies = []
    for piece, source, offset in plan:
        ref = pieces[piece] if source is None else pieces[piece].at[source]
        slot = lax.rem(at_ref[0] + offset, size)
        for t in range(times):
            target = out.at[slot] if times == 1 else out.at[t, slot]
            copies.append(pltpu.make_async_copy(ref, target, sem.at[len(copies)]))
            copies[-1].start()
    for copy in copies:
        copy.wait()


def pack(at, pieces, plan, times):
    size = len(plan)
    shape = (size, *pieces[-1].shape) if times == 1 else (times, size, *pieces[-1].shape)
    moved = 2 * times * size * pieces[-1].size
    return pl.pallas_call(
        lambda *refs: pack_kernel(*refs, plan=plan, size=size, times=times),
        out_shape=jax.ShapeDtypeStruct(shape, jnp.bfloat16),
        in_specs=[pl.BlockSpec(memory_space=pltpu.SMEM)]
        + [pl.BlockSpec(memory_space=pltpu.VMEM)] * len(pieces),
        out_specs=pl.BlockSpec(memory_space=pl.ANY),
        scratch_shapes=[pltpu.SemaphoreType.DMA((size * times,))],
        cost_estimate=pl.CostEstimate(
            flops=1_000_000_000, bytes_accessed=2 * moved, transcendentals=0
        ),
    )(at, *pieces)


Z_PLAN = [(0, 0, 0), (0, 1, 4), (1, 0, 7), (1, 1, 3), (2, 0, 1), (2, 1, 5), (3, None, 6), (4, None, 2)]


def shift_z(part, by):
    around = 2 * NZ
    return lax.ppermute(part, ("zh", "zl"), [(i, (i + by) % around) for i in range(around)])


def around_z(part):
    pair = jnp.stack([part, shift_z(part, 4)])
    low, high = shift_z(pair, 1), shift_z(pair, -1)
    return pair, low, high, shift_z(low[0], 1), shift_z(high[0], -1)


def squared(acc):
    acc = jnp.maximum(acc, 0.0)
    return (acc * acc).astype(jnp.bfloat16)


def down_part(hidden, held, out):
    f = hidden.shape[2]
    for at in range(0, out.shape[1], 512):
        acc = None
        for h in range(2):
            w = held[h, at : at + 512, f:]
            term = lax.dot_general(hidden[h], w, NT, preferred_element_type=jnp.float32)
            acc = term if acc is None else acc + term
        out[:, at : at + 512] = acc.astype(jnp.bfloat16)


def mixer_kernel(x_ref, w_ref, out, held, hidden, sem):
    f = hidden.shape[2]
    copies = []
    for side in range(2):
        for h in range(2):
            at = pl.ds(side * f, f)
            copies.append(pltpu.make_async_copy(w_ref.at[h, :, at], held.at[h, :, at], sem.at[side, h]))
            copies[-1].start()
    for h in range(2):
        copies[h].wait()
        hidden[h] = squared(jnp.dot(x_ref[...], held[h, :, :f], preferred_element_type=jnp.float32))
    for copy in copies[2:]:
        copy.wait()
    down_part(hidden, held, out)


def channel_mixer(x, w):
    rows, width = x.shape
    f = w.shape[2] // 2
    vmem = pl.BlockSpec(memory_space=pltpu.VMEM)
    return pl.pallas_call(
        mixer_kernel,
        out_shape=jax.ShapeDtypeStruct((rows, width), jnp.bfloat16),
        in_specs=[vmem, pl.BlockSpec(memory_space=pl.ANY)],
        out_specs=vmem,
        scratch_shapes=[
            pltpu.VMEM(w.shape, jnp.bfloat16),
            pltpu.VMEM((2, rows, f), jnp.bfloat16),
            pltpu.SemaphoreType.DMA((2, 2)),
        ],
        compiler_params=pltpu.CompilerParams(vmem_limit_bytes=58 * 1024 * 1024),
        cost_estimate=pl.CostEstimate(
            flops=8 * rows * width * f, bytes_accessed=2 * w.size, transcendentals=0
        ),
    )(x, w)


def body(
    tokens,
    mix_gain,
    gate_proj,
    value_proj,
    value_gain,
    value_shift,
    spatial_weight,
    spatial_shift,
    out_proj,
    ffn_gain,
    up_proj,
    down_proj,
):
    x, c = lax.axis_index("x"), lax.axis_index("c")
    at_z = jnp.reshape(lax.axis_index("zl"), (1,)).astype(jnp.int32)
    rows = tokens.shape[0] // 2
    width = tokens.shape[1]
    chunk = rows // NX
    k, n = gate_proj.shape
    f = up_proj.shape[1]

    part = jnp.concatenate([value_proj, gate_proj, out_proj.T], axis=1)
    small = exchange(pack(at_z, around_z(part), Z_PLAN, NY), "y")
    small = small.reshape(width, part.shape[1])
    small_w = (small, swap(small))

    half = f // 2
    at_half = lax.axis_index("zh") * half
    part = jnp.concatenate(
        [
            lax.dynamic_slice_in_dim(up_proj, at_half, half, 1),
            lax.dynamic_slice_in_dim(down_proj, at_half, half, 0).T,
        ],
        axis=1,
    )
    block = everyone(part, "y", NY).reshape(NY * k, f)
    large = lax.all_gather(block, ("zh", "zl"), axis=0, tiled=True).reshape(2, width, f)

    mine = lax.dynamic_slice_in_dim(tokens, c * rows, rows, 0)
    affine = jnp.stack([value_gain, value_shift])
    affine = jnp.concatenate([affine, swap(affine)], axis=1)

    normed = rms_norm(y_major(mine), y_major(mix_gain))
    value = jnp.concatenate(
        [jax.nn.gelu(jnp.dot(normed, w[:, :n], preferred_element_type=jnp.float32)) for w in small_w], axis=1
    )
    stats = jnp.stack([jnp.sum(value, axis=-1), jnp.sum(value * value, axis=-1)])
    stats = jnp.sum(everyone(stats, "x", NX), axis=0)
    gate = jnp.concatenate(
        [jax.nn.gelu(jnp.dot(normed, w[:, n : 2 * n], preferred_element_type=jnp.float32)) for w in small_w],
        axis=1,
    )
    centre = (stats[0] / GW)[:, None]
    spread = (stats[1] / GW)[:, None] - centre * centre
    leveled = ((value - centre) * lax.rsqrt(spread + EPS) * affine[0] + affine[1]).astype(jnp.bfloat16)
    lower = jnp.tril(lax.dynamic_index_in_dim(spatial_weight, x, 0, keepdims=False))
    offset = lax.dynamic_index_in_dim(spatial_shift, x, 0, keepdims=False)
    pieces = leveled.reshape(rows // BLOCK, BLOCK, 2 * n)
    mixed = (
        jnp.einsum("ts,nsw->ntw", lower, pieces, preferred_element_type=jnp.float32)
        + offset[None, :, None]
    )
    gated = (gate * mixed.reshape(rows, 2 * n)).astype(jnp.bfloat16)
    out_w = jnp.concatenate([w[:, 2 * n :] for w in small_w], axis=1)
    out_w = out_w.reshape(NY, NZ, k, 2 * n).transpose(1, 0, 2, 3).reshape(width, 2 * n)
    mixer = lax.dot_general(gated, out_w, NT, preferred_element_type=jnp.float32)
    mixer = mixer.astype(jnp.bfloat16).reshape(NX, chunk, width)
    mixer = jnp.sum(exchange(mixer, "x").astype(jnp.float32), axis=0)
    base = lax.dynamic_slice_in_dim(mine, x * chunk, chunk, 0)
    midway = (base.astype(jnp.float32) + mixer).astype(jnp.bfloat16)
    normed2 = everyone(rms_norm(midway, ffn_gain), "x", NX).reshape(rows, width)

    theirs = channel_mixer(swap(normed2), large)
    theirs = swap(theirs)
    terms = channel_mixer(normed2, large)
    terms = (terms.astype(jnp.float32) + theirs.astype(jnp.float32)).astype(jnp.bfloat16)
    ffn = jnp.sum(exchange(terms.reshape(NX, chunk, width), "x").astype(jnp.float32), axis=0)
    done = (midway.astype(jnp.float32) + ffn).astype(jnp.bfloat16)
    done = everyone(done, "x", NX).reshape(rows, width)
    at_c = jnp.reshape(c, (1,)).astype(jnp.int32)
    both = (done, swap(done))
    return pack(at_c, both, [(0, None, 0), (1, None, 1)], 1).reshape(2 * rows, width)


def solution(mesh):
    finer = Mesh(
        mesh.devices.reshape(mesh.shape["rep"], NZ, NY, NX, 2), ("zh", "zl", "y", "x", "c")
    )
    placed = (
        P(REP_FS, None),
        P(),
        P(FS, TP),
        P(FS, TP),
        P(TP),
        P(TP),
        P(),
        P(),
        P(TP, FS),
        P(),
        P(FS, TP),
        P(TP, FS),
    )

    return jax.shard_map(body, mesh=finer, in_specs=placed, out_specs=P(REP_FS, None), check_vma=False)
```

```python
import jax
import jax.numpy as jnp
from jax import lax
from jax.experimental import pallas as pl
from jax.experimental.pallas import tpu as pltpu
from jax.sharding import Mesh
from jax.sharding import PartitionSpec as P

GW = 1024
BLOCK = 128
EPS = 1e-06
FS = ("zl", "y")
TP = ("x", "c")
REP_FS = ("zh", "zl", "y")
NZ, NY, NX = 8, 4, 4
NT = (((1,), (1,)), ((), ()))


def rms_norm(values, scale):
    floats = values.astype(jnp.float32)
    return (
        floats * lax.rsqrt(jnp.mean(floats * floats, axis=-1, keepdims=True) + EPS) * scale
    ).astype(jnp.bfloat16)


def exchange(parts, axis):
    return lax.all_to_all(parts, axis, 0, 0, tiled=True)


def everyone(part, axis, size):
    return exchange(jnp.broadcast_to(part[None], (size, *part.shape)), axis)


def swap(part):
    return lax.ppermute(part, "c", [(0, 1), (1, 0)])


def y_major(array):
    k = array.shape[-1] // (NZ * NY)
    starts = [(z * NY + y) * k for y in range(NY) for z in range(NZ)]
    return jnp.concatenate([array[..., s : s + k] for s in starts], axis=-1)


def pack_kernel(at_ref, *refs, plan, size, times):
    pieces, out, sem = refs[:-2], refs[-2], refs[-1]
    copies = []
    for piece, source, offset in plan:
        ref = pieces[piece] if source is None else pieces[piece].at[source]
        slot = lax.rem(at_ref[0] + offset, size)
        for t in range(times):
            target = out.at[slot] if times == 1 else out.at[t, slot]
            copies.append(pltpu.make_async_copy(ref, target, sem.at[len(copies)]))
            copies[-1].start()
    for copy in copies:
        copy.wait()


def pack(at, pieces, plan, times):
    size = len(plan)
    shape = (size, *pieces[-1].shape) if times == 1 else (times, size, *pieces[-1].shape)
    moved = 2 * times * size * pieces[-1].size
    return pl.pallas_call(
        lambda *refs: pack_kernel(*refs, plan=plan, size=size, times=times),
        out_shape=jax.ShapeDtypeStruct(shape, jnp.bfloat16),
        in_specs=[pl.BlockSpec(memory_space=pltpu.SMEM)]
        + [pl.BlockSpec(memory_space=pltpu.VMEM)] * len(pieces),
        out_specs=pl.BlockSpec(memory_space=pl.ANY),
        scratch_shapes=[pltpu.SemaphoreType.DMA((size * times,))],
        cost_estimate=pl.CostEstimate(
            flops=1_000_000_000, bytes_accessed=2 * moved, transcendentals=0
        ),
    )(at, *pieces)


Z_PLAN = [(0, 0, 0), (0, 1, 4), (1, 0, 7), (1, 1, 3), (2, 0, 1), (2, 1, 5), (3, None, 6), (4, None, 2)]


def shift_z(part, by):
    around = 2 * NZ
    return lax.ppermute(part, ("zh", "zl"), [(i, (i + by) % around) for i in range(around)])


def around_z(part):
    pair = jnp.stack([part, shift_z(part, 4)])
    low, high = shift_z(pair, 1), shift_z(pair, -1)
    near_low = low[0]
    return pair, low, high, shift_z(near_low, 1), shift_z(high[0], -1)


def squared(acc):
    acc = jnp.maximum(acc, 0.0)
    return (acc * acc).astype(jnp.bfloat16)


def down_part(hidden, held, out):
    f = hidden.shape[2]
    for at in range(0, out.shape[1], 512):
        acc = None
        for h in range(2):
            w = held[h, at : at + 512, f:]
            term = lax.dot_general(hidden[h], w, NT, preferred_element_type=jnp.float32)
            acc = term if acc is None else acc + term
        out[:, at : at + 512] = acc.astype(jnp.bfloat16)


def mixer_kernel(x_ref, w_ref, out, hidden):
    f = hidden.shape[2]
    for h in range(2):
        hidden[h] = squared(jnp.dot(x_ref[...], w_ref[h, :, :f], preferred_element_type=jnp.float32))
    down_part(hidden, w_ref, out)


def channel_mixer(x, w):
    rows, width = x.shape
    f = w.shape[2] // 2
    return pl.pallas_call(
        mixer_kernel,
        out_shape=jax.ShapeDtypeStruct((rows, width), jnp.bfloat16),
        in_specs=[pl.BlockSpec(memory_space=pltpu.VMEM)] * 2,
        out_specs=pl.BlockSpec(memory_space=pltpu.VMEM),
        scratch_shapes=[pltpu.VMEM((2, rows, f), jnp.bfloat16)],
        compiler_params=pltpu.CompilerParams(vmem_limit_bytes=30 * 1024 * 1024),
        cost_estimate=pl.CostEstimate(
            flops=8 * rows * width * f, bytes_accessed=2 * w.size, transcendentals=0
        ),
    )(x, w)


def body(
    tokens,
    mix_gain,
    gate_proj,
    value_proj,
    value_gain,
    value_shift,
    spatial_weight,
    spatial_shift,
    out_proj,
    ffn_gain,
    up_proj,
    down_proj,
):
    x, c = lax.axis_index("x"), lax.axis_index("c")
    at_z = jnp.reshape(lax.axis_index("zl"), (1,)).astype(jnp.int32)
    rows = tokens.shape[0] // 2
    width = tokens.shape[1]
    chunk = rows // NX
    k, n = gate_proj.shape
    f = up_proj.shape[1]

    part = jnp.concatenate([value_proj, gate_proj, out_proj.T], axis=1)
    small = exchange(pack(at_z, around_z(part), Z_PLAN, NY), "y")
    small = small.reshape(width, part.shape[1])
    small_w = (small, swap(small))

    half = f // 2
    at_half = lax.axis_index("zh") * half
    part = jnp.concatenate(
        [
            lax.dynamic_slice_in_dim(up_proj, at_half, half, 1),
            lax.dynamic_slice_in_dim(down_proj, at_half, half, 0).T,
        ],
        axis=1,
    )
    block = everyone(part, "y", NY).reshape(NY * k, f)
    large = lax.all_gather(block, ("zh", "zl"), axis=0, tiled=True).reshape(2, width, f)

    mine = lax.dynamic_slice_in_dim(tokens, c * rows, rows, 0)
    affine = jnp.stack([value_gain, value_shift])
    affine = jnp.concatenate([affine, swap(affine)], axis=1)

    normed = rms_norm(y_major(mine), y_major(mix_gain))
    value = jnp.concatenate(
        [jax.nn.gelu(jnp.dot(normed, w[:, :n], preferred_element_type=jnp.float32)) for w in small_w], axis=1
    )
    stats = jnp.stack([jnp.sum(value, axis=-1), jnp.sum(value * value, axis=-1)])
    stats = jnp.sum(everyone(stats, "x", NX), axis=0)
    gate = jnp.concatenate(
        [jax.nn.gelu(jnp.dot(normed, w[:, n : 2 * n], preferred_element_type=jnp.float32)) for w in small_w],
        axis=1,
    )
    centre = (stats[0] / GW)[:, None]
    spread = (stats[1] / GW)[:, None] - centre * centre
    leveled = ((value - centre) * lax.rsqrt(spread + EPS) * affine[0] + affine[1]).astype(jnp.bfloat16)
    lower = jnp.tril(lax.dynamic_index_in_dim(spatial_weight, x, 0, keepdims=False))
    offset = lax.dynamic_index_in_dim(spatial_shift, x, 0, keepdims=False)
    pieces = leveled.reshape(rows // BLOCK, BLOCK, 2 * n)
    mixed = (
        jnp.einsum("ts,nsw->ntw", lower, pieces, preferred_element_type=jnp.float32)
        + offset[None, :, None]
    )
    gated = (gate * mixed.reshape(rows, 2 * n)).astype(jnp.bfloat16)
    out_w = jnp.concatenate([w[:, 2 * n :] for w in small_w], axis=1)
    out_w = out_w.reshape(NY, NZ, k, 2 * n).transpose(1, 0, 2, 3).reshape(width, 2 * n)
    mixer = lax.dot_general(gated, out_w, NT, preferred_element_type=jnp.float32)
    mixer = mixer.astype(jnp.bfloat16).reshape(NX, chunk, width)
    mixer = jnp.sum(exchange(mixer, "x").astype(jnp.float32), axis=0)
    base = lax.dynamic_slice_in_dim(mine, x * chunk, chunk, 0)
    midway = (base.astype(jnp.float32) + mixer).astype(jnp.bfloat16)
    normed2 = everyone(rms_norm(midway, ffn_gain), "x", NX).reshape(rows, width)

    theirs = channel_mixer(swap(normed2), large)
    theirs = swap(theirs)
    terms = channel_mixer(normed2, large)
    terms = (terms.astype(jnp.float32) + theirs.astype(jnp.float32)).astype(jnp.bfloat16)
    ffn = jnp.sum(exchange(terms.reshape(NX, chunk, width), "x").astype(jnp.float32), axis=0)
    done = (midway.astype(jnp.float32) + ffn).astype(jnp.bfloat16)
    done = everyone(done, "x", NX).reshape(rows, width)
    return everyone(done, "c", 2).reshape(2 * rows, width)


def solution(mesh):
    finer = Mesh(
        mesh.devices.reshape(mesh.shape["rep"], NZ, NY, NX, 2), ("zh", "zl", "y", "x", "c")
    )
    placed = (
        P(REP_FS, None),
        P(),
        P(FS, TP),
        P(FS, TP),
        P(TP),
        P(TP),
        P(),
        P(),
        P(TP, FS),
        P(),
        P(FS, TP),
        P(TP, FS),
    )

    return jax.shard_map(body, mesh=finer, in_specs=placed, out_specs=P(REP_FS, None), check_vma=False)
```

```python
import jax
import jax.numpy as jnp
from jax import lax
from jax.experimental import pallas as pl
from jax.experimental.pallas import tpu as pltpu
from jax.sharding import Mesh
from jax.sharding import PartitionSpec as P

GW = 1024
BLOCK = 128
EPS = 1e-06
FS = ("zl", "y")
TP = ("x", "c")
REP_FS = ("zh", "zl", "y")
NZ, NY, NX = 8, 4, 4
NT = (((1,), (1,)), ((), ()))


def rms_norm(values, scale):
    floats = values.astype(jnp.float32)
    return (
        floats * lax.rsqrt(jnp.mean(floats * floats, axis=-1, keepdims=True) + EPS) * scale
    ).astype(jnp.bfloat16)


def exchange(parts, axis):
    return lax.all_to_all(parts, axis, 0, 0, tiled=True)


def everyone(part, axis, size):
    return exchange(jnp.broadcast_to(part[None], (size, *part.shape)), axis)


def swap(part):
    return lax.ppermute(part, "c", [(0, 1), (1, 0)])


def y_major(array):
    k = array.shape[-1] // (NZ * NY)
    starts = [(z * NY + y) * k for y in range(NY) for z in range(NZ)]
    return jnp.concatenate([array[..., s : s + k] for s in starts], axis=-1)


def copy_kernel(at_ref, *refs, pieces, plan):
    sem = refs[-1]
    copies = []
    for source, target in plan(at_ref[0], refs[:pieces], refs[pieces:-1]):
        copies.append(pltpu.make_async_copy(source, target, sem.at[len(copies)]))
        copies[-1].start()
    for copy in copies:
        copy.wait()


def copied(at, pieces, plan, shapes, count):
    moved = 4 * sum(piece.size for piece in pieces)
    return pl.pallas_call(
        lambda *refs: copy_kernel(*refs, pieces=len(pieces), plan=plan),
        out_shape=tuple(jax.ShapeDtypeStruct(shape, jnp.bfloat16) for shape in shapes),
        in_specs=[pl.BlockSpec(memory_space=pltpu.SMEM)]
        + [pl.BlockSpec(memory_space=pltpu.VMEM)] * len(pieces),
        out_specs=tuple(pl.BlockSpec(memory_space=pl.ANY) for _ in shapes),
        scratch_shapes=[pltpu.SemaphoreType.DMA((count,))],
        cost_estimate=pl.CostEstimate(flops=1_000_000_000, bytes_accessed=moved, transcendentals=0),
    )(at, *pieces)


Y_OFFSETS = 0, 2, 3, 1


def around_y(part):
    moved = [part]
    for by in (2, 1, -1):
        moved.append(lax.ppermute(part, "y", [(i, (i + by) % NY) for i in range(NY)]))
    return moved


def pack_plan(y, pieces, outs):
    for piece, offset in zip(pieces, Y_OFFSETS):
        yield piece, outs[0].at[lax.rem(y + offset, NY)]


def late_plan(y, pieces, outs):
    for piece, offset in zip(pieces, Y_OFFSETS):
        yield piece, outs[0].at[:, lax.rem(y + offset, NY)]


def small_plan(z, pieces, outs):
    small, late = outs
    n = small.shape[3]
    for piece, source, offset in Z_PLAN:
        ref = pieces[piece] if source is None else pieces[piece].at[source]
        slot = lax.rem(z + offset, NZ)
        yield ref.at[:, pl.ds(n, late.shape[2])], late.at[slot]
        for t in range(NY):
            yield ref.at[:, pl.ds(0, n)], small.at[t, slot]


Z_PLAN = [(0, 0, 0), (0, 1, 4), (1, 0, 7), (1, 1, 3), (2, 0, 1), (2, 1, 5), (3, None, 6), (4, None, 2)]


def shift_z(part, by):
    around = 2 * NZ
    return lax.ppermute(part, ("zh", "zl"), [(i, (i + by) % around) for i in range(around)])


def around_z(part):
    pair = jnp.stack([part, shift_z(part, 4)])
    low, high = shift_z(pair, 1), shift_z(pair, -1)
    near_low = low[0]
    return pair, low, high, shift_z(near_low, 1), shift_z(high[0], -1)


def squared(acc):
    acc = jnp.maximum(acc, 0.0)
    return (acc * acc).astype(jnp.bfloat16)


def mixer_kernel(x_ref, w_ref, tail_ref, out, *hidden):
    weights = [(w_ref.at[h], hidden[h]) for h in range(2)] + [(tail_ref, hidden[2])]
    for w, units in weights:
        f = units.shape[1]
        units[...] = squared(jnp.dot(x_ref[...], w[:, :f], preferred_element_type=jnp.float32))
    for at in range(0, out.shape[1], 512):
        acc = None
        for w, units in weights:
            part = w[at : at + 512, units.shape[1] :]
            term = lax.dot_general(units[...], part, NT, preferred_element_type=jnp.float32)
            acc = term if acc is None else acc + term
        out[:, at : at + 512] = acc.astype(jnp.bfloat16)


def channel_mixer(x, w, tail):
    rows, width = x.shape
    f, late = w.shape[2] // 2, tail.shape[1] // 2
    return pl.pallas_call(
        mixer_kernel,
        out_shape=jax.ShapeDtypeStruct((rows, width), jnp.bfloat16),
        in_specs=[pl.BlockSpec(memory_space=pltpu.VMEM)] * 3,
        out_specs=pl.BlockSpec(memory_space=pltpu.VMEM),
        scratch_shapes=[pltpu.VMEM((rows, units), jnp.bfloat16) for units in (f, f, late)],
        compiler_params=pltpu.CompilerParams(vmem_limit_bytes=30 * 1024 * 1024),
        cost_estimate=pl.CostEstimate(
            flops=4 * rows * width * (2 * f + late),
            bytes_accessed=2 * (w.size + tail.size),
            transcendentals=0,
        ),
    )(x, w, tail)


def body(
    tokens,
    mix_gain,
    gate_proj,
    value_proj,
    value_gain,
    value_shift,
    spatial_weight,
    spatial_shift,
    out_proj,
    ffn_gain,
    up_proj,
    down_proj,
):
    x, c = lax.axis_index("x"), lax.axis_index("c")
    at_y = jnp.reshape(lax.axis_index("y"), (1,)).astype(jnp.int32)
    at_z = jnp.reshape(lax.axis_index("zl"), (1,)).astype(jnp.int32)
    rows = tokens.shape[0] // 2
    width = tokens.shape[1]
    chunk = rows // NX
    k, n = gate_proj.shape
    f = up_proj.shape[1]

    late = f // 4
    half = (f - late) // 2
    down_t = down_proj.T
    at_half = lax.axis_index("zh") * half
    part = jnp.concatenate(
        [lax.dynamic_slice_in_dim(w, at_half, half, 1) for w in (up_proj, down_t)], axis=1
    )
    shape = (NY, k, 2 * half)
    (block,) = copied(at_y, around_y(part), pack_plan, (shape,), NY)
    large = lax.all_gather(block.reshape(NY * k, 2 * half), ("zh", "zl"), axis=0, tiled=True)
    large = large.reshape(2, width, 2 * half)

    part = jnp.concatenate(
        [value_proj, gate_proj, out_proj.T, up_proj[:, f - late :], down_t[:, f - late :]], axis=1
    )
    shapes = (NY, NZ, k, 3 * n), (NZ, k, 2 * late)
    small, late_part = copied(at_z, around_z(part), small_plan, shapes, NZ * (NY + 1))
    small = exchange(small, "y").reshape(width, 3 * n)
    small_w = (small, swap(small))
    shape = (NZ, NY, k, 2 * late)
    (tail_w,) = copied(at_y, around_y(late_part), late_plan, (shape,), NY)
    tail_w = tail_w.reshape(width, 2 * late)

    mine = lax.dynamic_slice_in_dim(tokens, c * rows, rows, 0)
    affine = jnp.stack([value_gain, value_shift])
    affine = jnp.concatenate([affine, swap(affine)], axis=1)

    normed = rms_norm(y_major(mine), y_major(mix_gain))
    value = jnp.concatenate(
        [jax.nn.gelu(jnp.dot(normed, w[:, :n], preferred_element_type=jnp.float32)) for w in small_w], axis=1
    )
    stats = jnp.stack([jnp.sum(value, axis=-1), jnp.sum(value * value, axis=-1)])
    stats = jnp.sum(everyone(stats, "x", NX), axis=0)
    gate = jnp.concatenate(
        [jax.nn.gelu(jnp.dot(normed, w[:, n : 2 * n], preferred_element_type=jnp.float32)) for w in small_w],
        axis=1,
    )
    centre = (stats[0] / GW)[:, None]
    spread = (stats[1] / GW)[:, None] - centre * centre
    leveled = ((value - centre) * lax.rsqrt(spread + EPS) * affine[0] + affine[1]).astype(jnp.bfloat16)
    lower = jnp.tril(lax.dynamic_index_in_dim(spatial_weight, x, 0, keepdims=False))
    offset = lax.dynamic_index_in_dim(spatial_shift, x, 0, keepdims=False)
    pieces = leveled.reshape(rows // BLOCK, BLOCK, 2 * n)
    mixed = (
        jnp.einsum("ts,nsw->ntw", lower, pieces, preferred_element_type=jnp.float32)
        + offset[None, :, None]
    )
    gated = (gate * mixed.reshape(rows, 2 * n)).astype(jnp.bfloat16)
    out_w = jnp.concatenate([w[:, 2 * n :] for w in small_w], axis=1)
    out_w = out_w.reshape(NY, NZ, k, 2 * n).transpose(1, 0, 2, 3).reshape(width, 2 * n)
    mixer = lax.dot_general(gated, out_w, NT, preferred_element_type=jnp.float32)
    mixer = mixer.astype(jnp.bfloat16).reshape(NX, chunk, width)
    mixer = jnp.sum(exchange(mixer, "x").astype(jnp.float32), axis=0)
    base = lax.dynamic_slice_in_dim(mine, x * chunk, chunk, 0)
    midway = (base.astype(jnp.float32) + mixer).astype(jnp.bfloat16)
    normed2 = everyone(rms_norm(midway, ffn_gain), "x", NX).reshape(rows, width)

    theirs = channel_mixer(swap(normed2), large, tail_w)
    theirs = swap(theirs)
    terms = channel_mixer(normed2, large, tail_w)
    terms = (terms.astype(jnp.float32) + theirs.astype(jnp.float32)).astype(jnp.bfloat16)
    ffn = jnp.sum(exchange(terms.reshape(NX, chunk, width), "x").astype(jnp.float32), axis=0)
    done = (midway.astype(jnp.float32) + ffn).astype(jnp.bfloat16)
    done = everyone(done, "x", NX).reshape(rows, width)
    return everyone(done, "c", 2).reshape(2 * rows, width)


def solution(mesh):
    finer = Mesh(
        mesh.devices.reshape(mesh.shape["rep"], NZ, NY, NX, 2), ("zh", "zl", "y", "x", "c")
    )
    placed = (
        P(REP_FS, None),
        P(),
        P(FS, TP),
        P(FS, TP),
        P(TP),
        P(TP),
        P(),
        P(),
        P(TP, FS),
        P(),
        P(FS, TP),
        P(TP, FS),
    )

    return jax.shard_map(body, mesh=finer, in_specs=placed, out_specs=P(REP_FS, None), check_vma=False)
```

```python
import jax
import jax.numpy as jnp
from jax import lax
from jax.experimental import pallas as pl
from jax.experimental.pallas import tpu as pltpu
from jax.sharding import Mesh
from jax.sharding import PartitionSpec as P

GW = 1024
BLOCK = 128
EPS = 1e-06
FS = ("zl", "y")
TP = ("x", "c")
REP_FS = ("zh", "zl", "y")
NZ, NY, NX = 8, 4, 4
NT = (((1,), (1,)), ((), ()))


def rms_norm(values, scale):
    floats = values.astype(jnp.float32)
    return (
        floats * lax.rsqrt(jnp.mean(floats * floats, axis=-1, keepdims=True) + EPS) * scale
    ).astype(jnp.bfloat16)


def exchange(parts, axis):
    return lax.all_to_all(parts, axis, 0, 0, tiled=True)


def everyone(part, axis, size):
    return exchange(jnp.broadcast_to(part[None], (size, *part.shape)), axis)


def swap(part):
    return lax.ppermute(part, "c", [(0, 1), (1, 0)])


def y_major(array):
    k = array.shape[-1] // (NZ * NY)
    starts = [(z * NY + y) * k for y in range(NY) for z in range(NZ)]
    return jnp.concatenate([array[..., s : s + k] for s in starts], axis=-1)


def pack_kernel(at_ref, *refs, plan, size, times):
    pieces, out, sem = refs[:-2], refs[-2], refs[-1]
    copies = []
    for piece, source, offset in plan:
        ref = pieces[piece] if source is None else pieces[piece].at[source]
        slot = lax.rem(at_ref[0] + offset, size)
        for t in range(times):
            target = out.at[slot] if times == 1 else out.at[t, slot]
            copies.append(pltpu.make_async_copy(ref, target, sem.at[len(copies)]))
            copies[-1].start()
    for copy in copies:
        copy.wait()


def pack(at, pieces, plan, times):
    size = len(plan)
    shape = (size, *pieces[-1].shape) if times == 1 else (times, size, *pieces[-1].shape)
    moved = 2 * times * size * pieces[-1].size
    return pl.pallas_call(
        lambda *refs: pack_kernel(*refs, plan=plan, size=size, times=times),
        out_shape=jax.ShapeDtypeStruct(shape, jnp.bfloat16),
        in_specs=[pl.BlockSpec(memory_space=pltpu.SMEM)]
        + [pl.BlockSpec(memory_space=pltpu.VMEM)] * len(pieces),
        out_specs=pl.BlockSpec(memory_space=pl.ANY),
        scratch_shapes=[pltpu.SemaphoreType.DMA((size * times,))],
        cost_estimate=pl.CostEstimate(
            flops=1_000_000_000, bytes_accessed=2 * moved, transcendentals=0
        ),
    )(at, *pieces)


Z_PLAN = [(0, 0, 0), (0, 1, 4), (1, 0, 7), (1, 1, 3), (2, 0, 1), (2, 1, 5), (3, None, 6), (4, None, 2)]


def shift_z(part, by):
    around = 2 * NZ
    return lax.ppermute(part, ("zh", "zl"), [(i, (i + by) % around) for i in range(around)])


def around_z(part):
    far = shift_z(part, 4)
    pair = jnp.stack([part, far])
    low, high = shift_z(pair, 1), shift_z(pair, -1)
    return pair, low, high, shift_z(low[0], 1), shift_z(high[0], -1)


def squared(acc):
    acc = jnp.maximum(acc, 0.0)
    return (acc * acc).astype(jnp.bfloat16)


def down_part(hidden, held, out):
    f = hidden.shape[2]
    for at in range(0, out.shape[1], 512):
        acc = None
        for h in range(2):
            w = held[h, at : at + 512, f:]
            term = lax.dot_general(hidden[h], w, NT, preferred_element_type=jnp.float32)
            acc = term if acc is None else acc + term
        out[:, at : at + 512] = acc.astype(jnp.bfloat16)


def mixer_kernel(x_ref, w_ref, out, hidden):
    f = hidden.shape[2]
    for h in range(2):
        hidden[h] = squared(jnp.dot(x_ref[...], w_ref[h, :, :f], preferred_element_type=jnp.float32))
    down_part(hidden, w_ref, out)


def channel_mixer(x, w):
    rows, width = x.shape
    f = w.shape[2] // 2
    return pl.pallas_call(
        mixer_kernel,
        out_shape=jax.ShapeDtypeStruct((rows, width), jnp.bfloat16),
        in_specs=[pl.BlockSpec(memory_space=pltpu.VMEM)] * 2,
        out_specs=pl.BlockSpec(memory_space=pltpu.VMEM),
        scratch_shapes=[pltpu.VMEM((2, rows, f), jnp.bfloat16)],
        compiler_params=pltpu.CompilerParams(vmem_limit_bytes=30 * 1024 * 1024),
        cost_estimate=pl.CostEstimate(
            flops=8 * rows * width * f, bytes_accessed=2 * w.size, transcendentals=0
        ),
    )(x, w)


def body(
    tokens,
    mix_gain,
    gate_proj,
    value_proj,
    value_gain,
    value_shift,
    spatial_weight,
    spatial_shift,
    out_proj,
    ffn_gain,
    up_proj,
    down_proj,
):
    x, c = lax.axis_index("x"), lax.axis_index("c")
    at_z = jnp.reshape(lax.axis_index("zl"), (1,)).astype(jnp.int32)
    rows = tokens.shape[0] // 2
    width = tokens.shape[1]
    chunk = rows // NX
    k, n = gate_proj.shape
    f = up_proj.shape[1]

    part = jnp.concatenate([value_proj, gate_proj, out_proj.T], axis=1)
    small = exchange(pack(at_z, around_z(part), Z_PLAN, NY), "y")
    small = small.reshape(width, part.shape[1])
    small_w = (small, swap(small))

    half = f // 2
    at_half = lax.axis_index("zh") * half
    part = jnp.concatenate(
        [
            lax.dynamic_slice_in_dim(up_proj, at_half, half, 1),
            lax.dynamic_slice_in_dim(down_proj, at_half, half, 0).T,
        ],
        axis=1,
    )
    block = everyone(part, "y", NY).reshape(NY * k, f)
    large = lax.all_gather(block, ("zh", "zl"), axis=0, tiled=True).reshape(2, width, f)

    mine = lax.dynamic_slice_in_dim(tokens, c * rows, rows, 0)
    affine = jnp.stack([value_gain, value_shift])
    affine = jnp.concatenate([affine, swap(affine)], axis=1)

    normed = rms_norm(y_major(mine), y_major(mix_gain))
    value = jnp.concatenate(
        [jax.nn.gelu(jnp.dot(normed, w[:, :n], preferred_element_type=jnp.float32)) for w in small_w], axis=1
    )
    stats = jnp.stack([jnp.sum(value, axis=-1), jnp.sum(value * value, axis=-1)])
    stats = jnp.sum(everyone(stats, "x", NX), axis=0)
    gate = jnp.concatenate(
        [jax.nn.gelu(jnp.dot(normed, w[:, n : 2 * n], preferred_element_type=jnp.float32)) for w in small_w],
        axis=1,
    )
    centre = (stats[0] / GW)[:, None]
    spread = (stats[1] / GW)[:, None] - centre * centre
    leveled = ((value - centre) * lax.rsqrt(spread + EPS) * affine[0] + affine[1]).astype(jnp.bfloat16)
    lower = jnp.tril(lax.dynamic_index_in_dim(spatial_weight, x, 0, keepdims=False))
    offset = lax.dynamic_index_in_dim(spatial_shift, x, 0, keepdims=False)
    pieces = leveled.reshape(rows // BLOCK, BLOCK, 2 * n)
    mixed = (
        jnp.einsum("ts,nsw->ntw", lower, pieces, preferred_element_type=jnp.float32)
        + offset[None, :, None]
    )
    gated = (gate * mixed.reshape(rows, 2 * n)).astype(jnp.bfloat16)
    out_w = jnp.concatenate([w[:, 2 * n :] for w in small_w], axis=1)
    out_w = out_w.reshape(NY, NZ, k, 2 * n).transpose(1, 0, 2, 3).reshape(width, 2 * n)
    mixer = lax.dot_general(gated, out_w, NT, preferred_element_type=jnp.float32)
    mixer = mixer.astype(jnp.bfloat16).reshape(NX, chunk, width)
    mixer = jnp.sum(exchange(mixer, "x").astype(jnp.float32), axis=0)
    base = lax.dynamic_slice_in_dim(mine, x * chunk, chunk, 0)
    midway = (base.astype(jnp.float32) + mixer).astype(jnp.bfloat16)
    normed2 = everyone(rms_norm(midway, ffn_gain), "x", NX).reshape(rows, width)

    theirs = channel_mixer(swap(normed2), large)
    theirs = swap(theirs)
    terms = channel_mixer(normed2, large)
    terms = (terms.astype(jnp.float32) + theirs.astype(jnp.float32)).astype(jnp.bfloat16)
    ffn = jnp.sum(exchange(terms.reshape(NX, chunk, width), "x").astype(jnp.float32), axis=0)
    done = (midway.astype(jnp.float32) + ffn).astype(jnp.bfloat16)
    done = everyone(done, "x", NX).reshape(rows, width)
    other = swap(done)
    ours = (jnp.arange(2) == c)[:, None, None]
    return jnp.where(ours, done[None], other[None]).reshape(2 * rows, width)


def solution(mesh):
    finer = Mesh(
        mesh.devices.reshape(mesh.shape["rep"], NZ, NY, NX, 2), ("zh", "zl", "y", "x", "c")
    )
    placed = (
        P(REP_FS, None),
        P(),
        P(FS, TP),
        P(FS, TP),
        P(TP),
        P(TP),
        P(),
        P(),
        P(TP, FS),
        P(),
        P(FS, TP),
        P(TP, FS),
    )

    return jax.shard_map(body, mesh=finer, in_specs=placed, out_specs=P(REP_FS, None), check_vma=False)
```

```python
import jax
import jax.numpy as jnp
from jax import lax
from jax.experimental import pallas as pl
from jax.experimental.pallas import tpu as pltpu
from jax.sharding import Mesh
from jax.sharding import PartitionSpec as P

GW = 1024
BLOCK = 128
EPS = 1e-06
FS = ("zl", "y")
TP = ("x", "c")
REP_FS = ("zh", "zl", "y")
NZ, NY, NX = 8, 4, 4
NT = (((1,), (1,)), ((), ()))


def rms_norm(values, scale):
    floats = values.astype(jnp.float32)
    return (
        floats * lax.rsqrt(jnp.mean(floats * floats, axis=-1, keepdims=True) + EPS) * scale
    ).astype(jnp.bfloat16)


def exchange(parts, axis):
    return lax.all_to_all(parts, axis, 0, 0, tiled=True)


def everyone(part, axis, size):
    return exchange(jnp.broadcast_to(part[None], (size, *part.shape)), axis)


def swap(part):
    return lax.ppermute(part, "c", [(0, 1), (1, 0)])


def y_major(array):
    k = array.shape[-1] // (NZ * NY)
    starts = [(z * NY + y) * k for y in range(NY) for z in range(NZ)]
    return jnp.concatenate([array[..., s : s + k] for s in starts], axis=-1)


def pack_kernel(at_ref, *refs, plan, size, times):
    pieces, out, sem = refs[:-2], refs[-2], refs[-1]
    copies = []
    for piece, source, offset in plan:
        ref = pieces[piece].at[source]
        slot = lax.rem(at_ref[0] + offset, size)
        for t in range(times):
            target = out.at[slot] if times == 1 else out.at[t, slot]
            copies.append(pltpu.make_async_copy(ref, target, sem.at[len(copies)]))
            copies[-1].start()
    for copy in copies:
        copy.wait()


def pack(at, pieces, plan, times):
    size = len(plan)
    shape = (size, *pieces[0].shape[1:]) if times == 1 else (times, size, *pieces[0].shape[1:])
    moved = times * size * pieces[0].size
    return pl.pallas_call(
        lambda *refs: pack_kernel(*refs, plan=plan, size=size, times=times),
        out_shape=jax.ShapeDtypeStruct(shape, jnp.bfloat16),
        in_specs=[pl.BlockSpec(memory_space=pltpu.SMEM)]
        + [pl.BlockSpec(memory_space=pltpu.VMEM)] * len(pieces),
        out_specs=pl.BlockSpec(memory_space=pl.ANY),
        scratch_shapes=[pltpu.SemaphoreType.DMA((size * times,))],
        cost_estimate=pl.CostEstimate(
            flops=1_000_000_000, bytes_accessed=2 * moved, transcendentals=0
        ),
    )(at, *pieces)


Z_PLAN = [(0, 0, 0), (0, 1, 4), (1, 0, 7), (1, 1, 3), (2, 0, 1), (2, 1, 5), (3, 0, 6), (3, 1, 2)]


def shift_z(part, by):
    around = 2 * NZ
    return lax.ppermute(part, ("zh", "zl"), [(i, (i + by) % around) for i in range(around)])


def around_z(part):
    pair = jnp.stack([part, shift_z(part, 4)])
    low2 = shift_z(pair, 2)
    high, low = shift_z(pair, -1), shift_z(pair, 1)
    return pair, low, high, low2


def squared(acc):
    acc = jnp.maximum(acc, 0.0)
    return (acc * acc).astype(jnp.bfloat16)


def down_part(hidden, held, out):
    f = hidden.shape[2]
    for at in range(0, out.shape[1], 512):
        acc = None
        for h in range(2):
            w = held[h, at : at + 512, f:]
            term = lax.dot_general(hidden[h], w, NT, preferred_element_type=jnp.float32)
            acc = term if acc is None else acc + term
        out[:, at : at + 512] = acc.astype(jnp.bfloat16)


def mixer_kernel(x_ref, w_ref, out, hidden):
    f = hidden.shape[2]
    for h in range(2):
        hidden[h] = squared(jnp.dot(x_ref[...], w_ref[h, :, :f], preferred_element_type=jnp.float32))
    down_part(hidden, w_ref, out)


def channel_mixer(x, w):
    rows, width = x.shape
    f = w.shape[2] // 2
    return pl.pallas_call(
        mixer_kernel,
        out_shape=jax.ShapeDtypeStruct((rows, width), jnp.bfloat16),
        in_specs=[pl.BlockSpec(memory_space=pltpu.VMEM)] * 2,
        out_specs=pl.BlockSpec(memory_space=pltpu.VMEM),
        scratch_shapes=[pltpu.VMEM((2, rows, f), jnp.bfloat16)],
        compiler_params=pltpu.CompilerParams(vmem_limit_bytes=30 * 1024 * 1024),
        cost_estimate=pl.CostEstimate(
            flops=8 * rows * width * f, bytes_accessed=2 * w.size, transcendentals=0
        ),
    )(x, w)


def body(
    tokens,
    mix_gain,
    gate_proj,
    value_proj,
    value_gain,
    value_shift,
    spatial_weight,
    spatial_shift,
    out_proj,
    ffn_gain,
    up_proj,
    down_proj,
):
    x, c = lax.axis_index("x"), lax.axis_index("c")
    at_z = jnp.reshape(lax.axis_index("zl"), (1,)).astype(jnp.int32)
    rows = tokens.shape[0] // 2
    width = tokens.shape[1]
    chunk = rows // NX
    k, n = gate_proj.shape
    f = up_proj.shape[1]

    part = lax.optimization_barrier(jnp.concatenate([value_proj, gate_proj, out_proj.T], axis=1))
    small = exchange(pack(at_z, around_z(part), Z_PLAN, NY), "y")
    small = small.reshape(width, part.shape[1])
    small_w = (small, swap(small))

    half = f // 2
    at_half = lax.axis_index("zh") * half
    part = jnp.concatenate(
        [
            lax.dynamic_slice_in_dim(up_proj, at_half, half, 1),
            lax.dynamic_slice_in_dim(down_proj, at_half, half, 0).T,
        ],
        axis=1,
    )
    block = everyone(part, "y", NY).reshape(NY * k, f)
    large = lax.all_gather(block, ("zh", "zl"), axis=0, tiled=True).reshape(2, width, f)

    mine = lax.dynamic_slice_in_dim(tokens, c * rows, rows, 0)
    affine = jnp.stack([value_gain, value_shift])
    affine = jnp.concatenate([affine, swap(affine)], axis=1)

    normed = rms_norm(y_major(mine), y_major(mix_gain))
    value = jnp.concatenate(
        [jax.nn.gelu(jnp.dot(normed, w[:, :n], preferred_element_type=jnp.float32)) for w in small_w], axis=1
    )
    stats = jnp.stack([jnp.sum(value, axis=-1), jnp.sum(value * value, axis=-1)])
    stats = jnp.sum(everyone(stats, "x", NX), axis=0)
    gate = jnp.concatenate(
        [jax.nn.gelu(jnp.dot(normed, w[:, n : 2 * n], preferred_element_type=jnp.float32)) for w in small_w],
        axis=1,
    )
    centre = (stats[0] / GW)[:, None]
    spread = (stats[1] / GW)[:, None] - centre * centre
    leveled = ((value - centre) * lax.rsqrt(spread + EPS) * affine[0] + affine[1]).astype(jnp.bfloat16)
    lower = jnp.tril(lax.dynamic_index_in_dim(spatial_weight, x, 0, keepdims=False))
    offset = lax.dynamic_index_in_dim(spatial_shift, x, 0, keepdims=False)
    pieces = leveled.reshape(rows // BLOCK, BLOCK, 2 * n)
    mixed = (
        jnp.einsum("ts,nsw->ntw", lower, pieces, preferred_element_type=jnp.float32)
        + offset[None, :, None]
    )
    gated = (gate * mixed.reshape(rows, 2 * n)).astype(jnp.bfloat16)
    out_w = jnp.concatenate([w[:, 2 * n :] for w in small_w], axis=1)
    out_w = out_w.reshape(NY, NZ, k, 2 * n).transpose(1, 0, 2, 3).reshape(width, 2 * n)
    mixer = lax.dot_general(gated, out_w, NT, preferred_element_type=jnp.float32)
    mixer = mixer.astype(jnp.bfloat16).reshape(NX, chunk, width)
    mixer = jnp.sum(exchange(mixer, "x").astype(jnp.float32), axis=0)
    base = lax.dynamic_slice_in_dim(mine, x * chunk, chunk, 0)
    midway = (base.astype(jnp.float32) + mixer).astype(jnp.bfloat16)
    normed2 = everyone(rms_norm(midway, ffn_gain), "x", NX).reshape(rows, width)

    theirs = channel_mixer(swap(normed2), large)
    theirs = swap(theirs)
    terms = channel_mixer(normed2, large)
    terms = (terms.astype(jnp.float32) + theirs.astype(jnp.float32)).astype(jnp.bfloat16)
    ffn = jnp.sum(exchange(terms.reshape(NX, chunk, width), "x").astype(jnp.float32), axis=0)
    done = (midway.astype(jnp.float32) + ffn).astype(jnp.bfloat16)
    done = everyone(done, "x", NX).reshape(rows, width)
    other = swap(done)
    ours = (jnp.arange(2) == c)[:, None, None]
    return jnp.where(ours, done[None], other[None]).reshape(2 * rows, width)


def solution(mesh):
    finer = Mesh(
        mesh.devices.reshape(mesh.shape["rep"], NZ, NY, NX, 2), ("zh", "zl", "y", "x", "c")
    )
    placed = (
        P(REP_FS, None),
        P(),
        P(FS, TP),
        P(FS, TP),
        P(TP),
        P(TP),
        P(),
        P(),
        P(TP, FS),
        P(),
        P(FS, TP),
        P(TP, FS),
    )

    return jax.shard_map(body, mesh=finer, in_specs=placed, out_specs=P(REP_FS, None), check_vma=False)
```

```python
import jax
import jax.numpy as jnp
from jax import lax
from jax.experimental import pallas as pl
from jax.experimental.pallas import tpu as pltpu
from jax.sharding import Mesh
from jax.sharding import PartitionSpec as P

GW = 1024
BLOCK = 128
EPS = 1e-06
FS = ("zl", "y")
TP = ("x", "c")
REP_FS = ("zh", "zl", "y")
NZ, NY, NX = 8, 4, 4
NT = (((1,), (1,)), ((), ()))


def rms_norm(values, scale):
    floats = values.astype(jnp.float32)
    return (
        floats * lax.rsqrt(jnp.mean(floats * floats, axis=-1, keepdims=True) + EPS) * scale
    ).astype(jnp.bfloat16)


def exchange(parts, axis):
    return lax.all_to_all(parts, axis, 0, 0, tiled=True)


def everyone(part, axis, size):
    return exchange(jnp.broadcast_to(part[None], (size, *part.shape)), axis)


def swap(part):
    return lax.ppermute(part, "c", [(0, 1), (1, 0)])


def y_major(array):
    k = array.shape[-1] // (NZ * NY)
    starts = [(z * NY + y) * k for y in range(NY) for z in range(NZ)]
    return jnp.concatenate([array[..., s : s + k] for s in starts], axis=-1)


def pack_kernel(at_ref, *refs, plan, size, times):
    pieces, out, sem = refs[:-2], refs[-2], refs[-1]
    copies = []
    for piece, source, offset in plan:
        ref = pieces[piece] if source is None else pieces[piece].at[source]
        slot = lax.rem(at_ref[0] + offset, size)
        for t in range(times):
            target = out.at[slot] if times == 1 else out.at[t, slot]
            copies.append(pltpu.make_async_copy(ref, target, sem.at[len(copies)]))
            copies[-1].start()
    for copy in copies:
        copy.wait()


def pack(at, pieces, plan, times):
    size = len(plan)
    shape = (size, *pieces[-1].shape) if times == 1 else (times, size, *pieces[-1].shape)
    moved = 2 * times * size * pieces[-1].size
    return pl.pallas_call(
        lambda *refs: pack_kernel(*refs, plan=plan, size=size, times=times),
        out_shape=jax.ShapeDtypeStruct(shape, jnp.bfloat16),
        in_specs=[pl.BlockSpec(memory_space=pltpu.SMEM)]
        + [pl.BlockSpec(memory_space=pltpu.VMEM)] * len(pieces),
        out_specs=pl.BlockSpec(memory_space=pl.ANY),
        scratch_shapes=[pltpu.SemaphoreType.DMA((size * times,))],
        cost_estimate=pl.CostEstimate(
            flops=1_000_000_000, bytes_accessed=2 * moved, transcendentals=0
        ),
    )(at, *pieces)


Z_PLAN = [(0, 0, 0), (0, 1, 4), (1, 0, 7), (1, 1, 3), (2, 0, 1), (2, 1, 5), (3, None, 6), (4, None, 2)]


def shift_z(part, by):
    around = 2 * NZ
    return lax.ppermute(part, ("zh", "zl"), [(i, (i + by) % around) for i in range(around)])


def around_z(part):
    far = shift_z(part, 4)
    low2, high2 = shift_z(part, 2), shift_z(part, -2)
    pair = jnp.stack([part, far])
    return pair, shift_z(pair, 1), shift_z(pair, -1), low2, high2


def squared(acc):
    acc = jnp.maximum(acc, 0.0)
    return (acc * acc).astype(jnp.bfloat16)


def down_part(hidden, held, out):
    f = hidden.shape[2]
    for at in range(0, out.shape[1], 512):
        acc = None
        for h in range(2):
            w = held[h, at : at + 512, f:]
            term = lax.dot_general(hidden[h], w, NT, preferred_element_type=jnp.float32)
            acc = term if acc is None else acc + term
        out[:, at : at + 512] = acc.astype(jnp.bfloat16)


def mixer_kernel(x_ref, w_ref, out, hidden):
    f = hidden.shape[2]
    for h in range(2):
        hidden[h] = squared(jnp.dot(x_ref[...], w_ref[h, :, :f], preferred_element_type=jnp.float32))
    down_part(hidden, w_ref, out)


def channel_mixer(x, w):
    rows, width = x.shape
    f = w.shape[2] // 2
    return pl.pallas_call(
        mixer_kernel,
        out_shape=jax.ShapeDtypeStruct((rows, width), jnp.bfloat16),
        in_specs=[pl.BlockSpec(memory_space=pltpu.VMEM)] * 2,
        out_specs=pl.BlockSpec(memory_space=pltpu.VMEM),
        scratch_shapes=[pltpu.VMEM((2, rows, f), jnp.bfloat16)],
        compiler_params=pltpu.CompilerParams(vmem_limit_bytes=30 * 1024 * 1024),
        cost_estimate=pl.CostEstimate(
            flops=8 * rows * width * f, bytes_accessed=2 * w.size, transcendentals=0
        ),
    )(x, w)


def body(
    tokens,
    mix_gain,
    gate_proj,
    value_proj,
    value_gain,
    value_shift,
    spatial_weight,
    spatial_shift,
    out_proj,
    ffn_gain,
    up_proj,
    down_proj,
):
    x, c = lax.axis_index("x"), lax.axis_index("c")
    at_z = jnp.reshape(lax.axis_index("zl"), (1,)).astype(jnp.int32)
    rows = tokens.shape[0] // 2
    width = tokens.shape[1]
    chunk = rows // NX
    k, n = gate_proj.shape
    f = up_proj.shape[1]

    part = lax.optimization_barrier(jnp.concatenate([value_proj, gate_proj, out_proj.T], axis=1))
    small = exchange(pack(at_z, around_z(part), Z_PLAN, NY), "y")
    small = small.reshape(width, part.shape[1])
    small_w = (small, swap(small))

    half = f // 2
    at_half = lax.axis_index("zh") * half
    part = jnp.concatenate(
        [
            lax.dynamic_slice_in_dim(up_proj, at_half, half, 1),
            lax.dynamic_slice_in_dim(down_proj, at_half, half, 0).T,
        ],
        axis=1,
    )
    block = everyone(part, "y", NY)
    block = jnp.where(at_z[0] < NZ, block, jnp.zeros_like(block)).reshape(NY * k, f)
    large = lax.all_gather(block, ("zh", "zl"), axis=0, tiled=True).reshape(2, width, f)

    mine = lax.dynamic_slice_in_dim(tokens, c * rows, rows, 0)
    affine = jnp.stack([value_gain, value_shift])
    affine = jnp.concatenate([affine, swap(affine)], axis=1)

    normed = rms_norm(y_major(mine), y_major(mix_gain))
    value = jnp.concatenate(
        [jax.nn.gelu(jnp.dot(normed, w[:, :n], preferred_element_type=jnp.float32)) for w in small_w], axis=1
    )
    stats = jnp.stack([jnp.sum(value, axis=-1), jnp.sum(value * value, axis=-1)])
    stats = jnp.sum(everyone(stats, "x", NX), axis=0)
    gate = jnp.concatenate(
        [jax.nn.gelu(jnp.dot(normed, w[:, n : 2 * n], preferred_element_type=jnp.float32)) for w in small_w],
        axis=1,
    )
    centre = (stats[0] / GW)[:, None]
    spread = (stats[1] / GW)[:, None] - centre * centre
    leveled = ((value - centre) * lax.rsqrt(spread + EPS) * affine[0] + affine[1]).astype(jnp.bfloat16)
    lower = jnp.tril(lax.dynamic_index_in_dim(spatial_weight, x, 0, keepdims=False))
    offset = lax.dynamic_index_in_dim(spatial_shift, x, 0, keepdims=False)
    pieces = leveled.reshape(rows // BLOCK, BLOCK, 2 * n)
    mixed = (
        jnp.einsum("ts,nsw->ntw", lower, pieces, preferred_element_type=jnp.float32)
        + offset[None, :, None]
    )
    gated = (gate * mixed.reshape(rows, 2 * n)).astype(jnp.bfloat16)
    out_w = jnp.concatenate([w[:, 2 * n :] for w in small_w], axis=1)
    out_w = out_w.reshape(NY, NZ, k, 2 * n).transpose(1, 0, 2, 3).reshape(width, 2 * n)
    mixer = lax.dot_general(gated, out_w, NT, preferred_element_type=jnp.float32)
    mixer = mixer.astype(jnp.bfloat16).reshape(NX, chunk, width)
    mixer = jnp.sum(exchange(mixer, "x").astype(jnp.float32), axis=0)
    base = lax.dynamic_slice_in_dim(mine, x * chunk, chunk, 0)
    midway = (base.astype(jnp.float32) + mixer).astype(jnp.bfloat16)
    normed2 = everyone(rms_norm(midway, ffn_gain), "x", NX).reshape(rows, width)

    theirs = channel_mixer(swap(normed2), large)
    theirs = swap(theirs)
    terms = channel_mixer(normed2, large)
    terms = (terms.astype(jnp.float32) + theirs.astype(jnp.float32)).astype(jnp.bfloat16)
    ffn = jnp.sum(exchange(terms.reshape(NX, chunk, width), "x").astype(jnp.float32), axis=0)
    done = (midway.astype(jnp.float32) + ffn).astype(jnp.bfloat16)
    done = everyone(done, "x", NX).reshape(rows, width)
    other = swap(done)
    ours = (jnp.arange(2) == c)[:, None, None]
    return jnp.where(ours, done[None], other[None]).reshape(2 * rows, width)


def solution(mesh):
    finer = Mesh(
        mesh.devices.reshape(mesh.shape["rep"], NZ, NY, NX, 2), ("zh", "zl", "y", "x", "c")
    )
    placed = (
        P(REP_FS, None),
        P(),
        P(FS, TP),
        P(FS, TP),
        P(TP),
        P(TP),
        P(),
        P(),
        P(TP, FS),
        P(),
        P(FS, TP),
        P(TP, FS),
    )

    return jax.shard_map(body, mesh=finer, in_specs=placed, out_specs=P(REP_FS, None), check_vma=False)
```
